512 devices in a mesh: sp: 64 (over z, y), tp: 8 (over x, core).
Axes of the slice: x: 4, y: 8, z: 8, core: 2. Of those that a mesh axis runs over, the one named last changes fastest.
Arguments:
- tokens: bfloat16 [8192, 2048], P('sp', 'tp'), may hold values from -6 to 6
- pre_gain: float32 [2048], replicated, may hold values from 0.1 to 1.9
- w_query_stick: bfloat16 [2048, 1024], P(None, 'tp'), may hold values from -0.125 to 0.125
- w_key_stick: bfloat16 [2048, 1024], P(None, 'tp'), may hold values from -0.125 to 0.125
- w_value_stick: bfloat16 [2048, 1024], P(None, 'tp'), may hold values from -2 to 2, as said below
- w_query_window: bfloat16 [2048, 1024], P(None, 'tp'), may hold values from -20 to 20, as said below
- w_key_window: bfloat16 [2048, 512], P(None, 'tp'), may hold values from -1 to 1, as said below
- w_value_window: bfloat16 [2048, 512], P(None, 'tp'), may hold values from -2 to 2, as said below
- stick_bias: float32 [16], P('tp'), may hold values from -14 to -3
- sinks: float32 [16], P('tp'), may hold values from 2 to 6
- stick_gain: float32 [1024], P('tp'), may hold values from 0.1 to 1.9
- window_gain: float32 [1024], P('tp'), may hold values from 0.1 to 1.9
- w_out_stick: bfloat16 [1024, 2048], P('tp'), may hold values from -0.125 to 0.125
- w_out_window: bfloat16 [1024, 2048], P('tp'), may hold values from -0.125 to 0.125
- post_gain: float32 [2048], replicated, may hold values from 0.1 to 1.9
Outputs:
- layer_out: bfloat16 [8192, 2048], P(('sp', 'tp'))
The draws below stay inside these ranges and needn't reach their ends.
Inputs may be any that keep to these rules, and one draw needn't show every extreme that they name: `w_key_window`: key weights of the windowed heads. `w_query_window`: query weights of the windowed heads. `w_value_stick`: value weights of the stick-breaking heads. `w_value_window`: value weights of the windowed heads.
All inputs are finite; a program needn't handle non-finite values.
Results may differ from the reference program's by a relative error of at most 0.018.
Values may be sent and summed in bfloat16 or wider, within the bound.
A program may use at most 64 MiB of HBM per device.

```python
import jax
import jax.numpy as jnp
from jax import lax

D = 2048
HEAD_DIM = 64
SB_HEADS = 16
SW_KV_HEADS = 8
GROUP = 2
WINDOW = 128
TOK_DEV = 128
TOKENS = 8192
SW_HEADS = 16
SB_WIDTH = 1024
SW_WIDTH = 1024


def clipped_normal(key, shape):
    return jnp.clip(jax.random.normal(key, shape, jnp.float32), -4.0, 4.0)


def window_pair(key):
    salted = jax.random.fold_in(key, 17)
    keys_w = clipped_normal(jax.random.fold_in(salted, 1), (D, SW_KV_HEADS * HEAD_DIM)) * D ** (-0.5)
    queries_w = clipped_normal(jax.random.fold_in(salted, 2), (D, SW_HEADS * HEAD_DIM)) * D ** (-0.5)
    return (keys_w, queries_w)


def draw_w_key_window(key, part):
    return window_pair(key)[0].astype(jnp.bfloat16)


def draw_w_query_window(key, part):
    keys_w, queries_w = window_pair(key)
    return queries_w.astype(jnp.bfloat16)


def scaled_values(key, salt, head_count):
    salted = jax.random.fold_in(key, salt)
    head_scale = jnp.exp(jax.random.uniform(jax.random.fold_in(salted, 1), (head_count,), jnp.float32, -1.2, 1.2))
    normals = clipped_normal(jax.random.fold_in(salted, 2), (D, head_count * HEAD_DIM)) * D ** (-0.5)
    return normals * jnp.repeat(head_scale, HEAD_DIM)[None, :]


def draw_w_value_stick(key, part):
    return scaled_values(key, 23, SB_HEADS).astype(jnp.bfloat16)


def draw_w_value_window(key, part):
    return scaled_values(key, 31, SW_KV_HEADS).astype(jnp.bfloat16)


def draw_stick_bias(key, part):
    salted = jax.random.fold_in(key, 29)
    slow_bias = -jnp.log(TOKENS * 1.0) - jax.random.uniform(jax.random.fold_in(salted, 1), (SB_HEADS,), jnp.float32, 0.0, 1.0)
    fast_bias = jax.random.uniform(jax.random.fold_in(salted, 2), (SB_HEADS,), jnp.float32, -4.0, -3.5)
    chosen = jax.random.permutation(jax.random.fold_in(salted, 3), SB_HEADS) < SB_HEADS // 2
    return jnp.where(chosen, slow_bias, fast_bias)


def steps_of(own_key, shape, split, smallest, high):
    def one(position, blocks):
        heights = jax.random.uniform(jax.random.fold_in(jax.random.fold_in(own_key, 6), position), (blocks,), jnp.float32, smallest / len(split), high / len(split))
        return jnp.repeat(jnp.exp(heights), shape[position] // blocks).reshape((-1,) + (1,) * (len(shape) - position - 1))

    level = one(*split[0])
    for cut in split[1:]:
        level = level * one(*cut)
    return level


def scatter_about(own_key, shape, width, most, split=(), held_as=jnp.bfloat16):
    values = width * jax.random.normal(own_key, shape, jnp.float32)
    if split:
        values = values * steps_of(own_key, shape, split, -0.22, 0.18)
    return jnp.clip(values, -most, most).astype(held_as)


def setup_inputs(seed: int = 0) -> dict:
    key_of = jax.random.split(jax.random.key(seed), 16)
    return {
        "tokens": scatter_about(key_of[0], (TOKENS, D), 1.0, 6.0, ((0, 64), (1, 8))),
        "pre_gain": jnp.clip(1.0 + 0.18 * jax.random.normal(key_of[1], (D,), jnp.float32), 0.1, 1.9),
        "w_query_stick": scatter_about(key_of[2], (D, SB_WIDTH), D ** -0.5, 0.125, ((1, 8),)),
        "w_key_stick": scatter_about(key_of[3], (D, SB_WIDTH), D ** -0.5, 0.125, ((1, 8),)),
        "w_value_stick": draw_w_value_stick(jax.random.fold_in(key_of[15], 71), 0),
        "w_query_window": draw_w_query_window(jax.random.fold_in(key_of[15], 71), 0),
        "w_key_window": draw_w_key_window(jax.random.fold_in(key_of[15], 71), 0),
        "w_value_window": draw_w_value_window(jax.random.fold_in(key_of[15], 71), 0),
        "stick_bias": draw_stick_bias(jax.random.fold_in(key_of[15], 71), 0),
        "sinks": jnp.clip(2.0 + 4.0 * jax.random.uniform(key_of[9], (SW_HEADS,), jnp.float32) ** steps_of(key_of[9], (SW_HEADS,), ((0, 8),), -0.2, 0.2), 2.0, 6.0),
        "stick_gain": jnp.clip(1.0 + 0.18 * jax.random.normal(key_of[10], (SB_WIDTH,), jnp.float32), 0.1, 1.9),
        "window_gain": jnp.clip(1.0 + 0.18 * jax.random.normal(key_of[11], (SW_WIDTH,), jnp.float32), 0.1, 1.9),
        "w_out_stick": scatter_about(key_of[12], (SB_WIDTH, D), (SB_WIDTH + SW_WIDTH) ** -0.5, 0.125, ((0, 8),)),
        "w_out_window": scatter_about(key_of[13], (SW_WIDTH, D), (SB_WIDTH + SW_WIDTH) ** -0.5, 0.125, ((0, 8),)),
        "post_gain": jnp.clip(1.0 + 0.18 * jax.random.normal(key_of[14], (D,), jnp.float32), 0.1, 1.9),
    }


epsilon = 1e-06

def rounded(values):
    return lax.optimization_barrier(values.astype(jnp.bfloat16)).astype(jnp.float32)

def norm_rows(values, gain):
    stats = lax.optimization_barrier(jnp.mean(values * values, axis=-1, keepdims=True))
    return values * lax.rsqrt(stats + epsilon) * gain

def stick_attention(queries, key_rows, values, stick_bias):
    blocks = TOKENS // TOK_DEV
    q_blocks = queries.reshape(blocks, TOK_DEV, SB_HEADS, HEAD_DIM).astype(jnp.float32)
    k_blocks = key_rows.reshape(blocks, TOK_DEV, SB_HEADS, HEAD_DIM).astype(jnp.float32)
    v_blocks = values.reshape(blocks, TOK_DEV, SB_HEADS, HEAD_DIM).astype(jnp.float32)
    offsets = jnp.arange(TOK_DEV, dtype=jnp.int32)
    scaling = HEAD_DIM ** (-0.5)

    def one_query(block_args):
        q_blk, q_index = block_args
        q_pos = q_index * TOK_DEV + offsets

        def key_step(carried, inputs):
            result, logsum = carried
            k_blk, v_blk, k_index = inputs
            k_pos = k_index * TOK_DEV + offsets
            before = (k_pos[None, :] < q_pos[:, None])[None]
            scores = jnp.einsum('thd,shd->hts', q_blk, k_blk) * scaling + stick_bias[:, None, None]
            log_keep = jnp.where(before, jax.nn.log_sigmoid(-scores), 0.0)
            suffix = lax.cumsum(log_keep, axis=2, reverse=True) - log_keep
            stick_weights = jnp.where(before, jnp.exp(jax.nn.log_sigmoid(scores) + suffix + logsum[:, :, None]), 0.0)
            stick_weights = rounded(stick_weights)
            result = result + jnp.einsum('hts,shd->htd', stick_weights, v_blk)
            logsum = logsum + lax.optimization_barrier(jnp.sum(log_keep, axis=2))
            return ((result, logsum), None)
        initial = (jnp.zeros((SB_HEADS, TOK_DEV, HEAD_DIM), jnp.float32), jnp.zeros((SB_HEADS, TOK_DEV), jnp.float32))
        (result, _), _ = lax.scan(key_step, initial, (k_blocks, v_blocks, jnp.arange(blocks, dtype=jnp.int32)), reverse=True)
        return result.transpose(1, 0, 2)
    outputs = lax.map(one_query, (q_blocks, jnp.arange(blocks, dtype=jnp.int32)))
    return outputs.reshape(TOKENS, SB_WIDTH).astype(jnp.bfloat16)

def window_attention(queries, key_rows, values, sinks):
    block_count = TOKENS // WINDOW
    q_blocks = queries.reshape(block_count, WINDOW, SW_KV_HEADS, GROUP, HEAD_DIM).astype(jnp.float32)
    k_heads = key_rows.reshape(block_count, WINDOW, SW_KV_HEADS, HEAD_DIM).astype(jnp.float32)
    v_heads = values.reshape(block_count, WINDOW, SW_KV_HEADS, HEAD_DIM).astype(jnp.float32)
    zero_block = jnp.zeros((1, WINDOW, SW_KV_HEADS, HEAD_DIM), jnp.float32)
    k_band = jnp.concatenate([jnp.concatenate([zero_block, k_heads[:-1]], axis=0), k_heads], axis=1)
    v_band = jnp.concatenate([jnp.concatenate([zero_block, v_heads[:-1]], axis=0), v_heads], axis=1)
    logits = jnp.einsum('nqhgd,nchd->nhgqc', q_blocks, k_band) * HEAD_DIM ** (-0.5)
    query_offs = jnp.arange(WINDOW, dtype=jnp.int32)[:, None]
    key_offs = jnp.arange(2 * WINDOW, dtype=jnp.int32)[None, :]
    distance = query_offs + WINDOW - key_offs
    key_pos = jnp.arange(block_count, dtype=jnp.int32)[:, None] * WINDOW - WINDOW + key_offs
    usable = ((distance >= 0) & (distance < WINDOW))[None] & (key_pos >= 0)[:, None, :]
    logits = jnp.where(usable[:, None, None], logits, -jnp.inf)
    sink_logit = sinks.reshape(SW_KV_HEADS, GROUP)[None, :, :, None, None]
    row_top = jnp.maximum(lax.optimization_barrier(jnp.max(logits, axis=-1, keepdims=True)), sink_logit)
    weights_exp = jnp.exp(logits - row_top)
    normalizer = lax.optimization_barrier(jnp.sum(weights_exp, axis=-1, keepdims=True)) + jnp.exp(sink_logit - row_top)
    window_weights = rounded(weights_exp / normalizer)
    result = jnp.einsum('nhgqc,nchd->nqhgd', window_weights, v_band)
    return result.reshape(TOKENS, SW_WIDTH).astype(jnp.bfloat16)

def reference(tokens, pre_gain, w_query_stick, w_key_stick, w_value_stick, w_query_window, w_key_window, w_value_window, stick_bias, sinks, stick_gain, window_gain, w_out_stick, w_out_window, post_gain):
    normed = norm_rows(tokens.astype(jnp.float32), pre_gain).astype(jnp.bfloat16)

    def project(weight):
        return jnp.dot(normed, weight, preferred_element_type=jnp.float32).astype(jnp.bfloat16)
    stick_out = stick_attention(project(w_query_stick), project(w_key_stick), project(w_value_stick), stick_bias)
    window_out = window_attention(project(w_query_window), project(w_key_window), project(w_value_window), sinks)
    stick_normed = norm_rows(stick_out.astype(jnp.float32), stick_gain).astype(jnp.bfloat16)
    window_normed = norm_rows(window_out.astype(jnp.float32), window_gain).astype(jnp.bfloat16)
    combined = jnp.dot(stick_normed, w_out_stick, preferred_element_type=jnp.float32)
    combined = combined + jnp.dot(window_normed, w_out_window, preferred_element_type=jnp.float32)
    combined = rounded(combined)
    return norm_rows(combined, post_gain).astype(jnp.bfloat16)
```

```python
import functools

import jax
import jax.numpy as jnp
from jax import lax
from jax.experimental import pallas as pl
from jax.experimental.pallas import tpu as pltpu
from jax.sharding import PartitionSpec as P

T = 128
D = 2048
CH = 256
NY = 8
NZ = 8
NTP = 8
NX = 4
LOG2E = 1.4426950408889634
EPS = 1e-06
PACK = D + 128
PROWS = T + 16
MESH = pl.DeviceIdType.MESH
F32 = jnp.float32
BF16 = jnp.bfloat16


def dot(a, b):
    return jnp.dot(a, b, preferred_element_type=F32)


def dot_nt(a, b):
    return lax.dot_general(a, b, (((1,), (1,)), ((), ())), preferred_element_type=F32)


def iota(shape, dim):
    return lax.broadcasted_iota(jnp.int32, shape, dim)


def with_squares(ref, out):
    total = jnp.sum(out * out, axis=1, keepdims=True)
    high = total.astype(BF16).astype(F32)
    lane = iota((T, 128), 1)
    ref[:, D:] = jnp.where(lane == 0, high, jnp.where(lane == 1, total - high, 0.0)).astype(BF16)


def kernel(
    tok, pre, wqs, wks, wvs, wqw, wkw, wvw, bias, sinks, sgain, wgain, wos, wow, post,
    out,
    tok_all, w4, wk6, wv6, wo_s, wo_w, pre_v, sg_v, wg_v, post_v,
    acc4, acck, accv, sq, kvb, qb, kbd, vbd, tri, ones,
    wkv, pwkv, pout, prec, acc_p, acc_l, ab, bb, ra, rb,
    lsem, s_a, r_a, s_k, r_k, r_k4, s_q, r_q, s_w, r_w, s_p, r_p, s_ra, r_ra, s_rb, r_rb,
):
    sp = lax.axis_index("sp")
    tp = lax.axis_index("tp")
    z = sp // NY
    y = sp % NY
    x = tp // 2
    c = tp % 2

    def rcopy(src, dst, ssem, rsem, dev):
        return pltpu.make_async_remote_copy(
            src_ref=src, dst_ref=dst, send_sem=ssem, recv_sem=rsem, device_id=dev, device_id_type=MESH
        )

    loads = [pltpu.make_async_copy(tok, tok_all.at[tp], lsem.at[0])]
    pairs = [
        (pre, pre_v), (wks, w4.at[:, pl.ds(0, 128)]), (wvs, w4.at[:, pl.ds(128, 128)]),
        (wqs, w4.at[:, pl.ds(256, 128)]), (wqw, w4.at[:, pl.ds(384, 128)]), (wkw, wk6), (wvw, wv6),
        (sgain, sg_v), (wgain, wg_v), (post, post_v), (wos, wo_s), (wow, wo_w),
    ]
    for n, (src, dst) in enumerate(pairs):
        loads.append(pltpu.make_async_copy(src, dst, lsem.at[n + 1]))
    for load in loads:
        load.start()

    barrier = pltpu.get_barrier_semaphore()
    greeted = [(sp, (tp + d) % NTP) for d in range(1, NTP)]
    greeted += [(z * NY + (y + d) % NY, tp) for d in (1, 2, NY - 2, NY - 1)]
    greeted += [(((z + d) % NZ) * NY + y, tp) for d in range(1, NZ)]
    greeted += [((sp + d) % (NY * NZ), tp) for d in (1, NY * NZ - 1)]
    for dev in greeted:
        pl.semaphore_signal(barrier, inc=1, device_id=dev, device_id_type=MESH)

    row2, col2 = iota((256, 256), 0), iota((256, 256), 1)
    tri[...] = jnp.where((row2 > col2) & (row2 // T == col2 // T), 1.0, 0.0).astype(BF16)
    ones[...] = jnp.where(iota((256, 128), 0) // T == iota((256, 128), 1) // 64, 1.0, 0.0).astype(BF16)
    acc4[...] = jnp.zeros_like(acc4)
    acck[...] = jnp.zeros_like(acck)
    accv[...] = jnp.zeros_like(accv)
    sq[...] = jnp.zeros_like(sq)

    pl.semaphore_wait(barrier, len(greeted))
    loads[0].wait()

    partner = x * 2 + (1 - c)
    own_tok = tok_all.at[tp]
    tok_sends = []
    for n, d in enumerate((2, 1, 3)):
        peer = ((x + d) % NX) * 2 + c
        tok_sends.append(rcopy(own_tok, own_tok, s_a.at[n], r_a.at[tp], (sp, peer)))
    tok_sends.append(rcopy(own_tok, own_tok, s_a.at[3], r_a.at[tp], (sp, partner)))
    for send in tok_sends:
        send.start()
    for load in loads[1:8]:
        load.wait()

    def feature_step(i, _):
        dist = jnp.where(i < 2, 0, jnp.where((i == 2) | (i == 5), 1, jnp.where((i == 3) | (i == 6), 3, 2)))
        core = jnp.where((i == 1) | (i >= 5), 1 - c, c)
        src = ((x + dist) % NX) * 2 + core
        block = tok_all.at[src]

        @pl.when(i > 0)
        def _():
            rcopy(block, block, s_a.at[0], r_a.at[src], (sp, partner)).wait_recv()

        @pl.when((i >= 2) & (i <= 4))
        def _():
            rcopy(block, block, s_a.at[i + 2], r_a.at[src], (sp, partner)).start()

        feats = block[...].astype(F32)
        sq[...] += feats[:, :128] * feats[:, :128] + feats[:, 128:] * feats[:, 128:]
        at = pl.ds(pl.multiple_of(src * CH, CH), CH)
        scaled = (feats * pre_v[:, at]).astype(BF16)
        acc4[...] += dot(scaled, w4[at, :])
        acck[...] += dot(scaled, wk6[at, :])
        accv[...] += dot(scaled, wv6[at, :])
        return 0

    lax.fori_loop(0, NTP, feature_step, 0)
    inv = lax.rsqrt(jnp.sum(sq[...], axis=1, keepdims=True) * (1.0 / D) + EPS)

    kvb[y, 0] = (acc4[:, 0:128] * inv).T.astype(BF16)
    kvb[y, 1] = (acc4[:, 128:256] * inv).astype(BF16)
    own_kv = kvb.at[y]
    kv_sends = []
    for n, d in enumerate((2, NY - 2, 1, NY - 1)):
        kv_sends.append(rcopy(own_kv, own_kv, s_k.at[n], r_k.at[y], (z * NY + (y + d) % NY, tp)))
    for send in kv_sends:
        send.start()
    qb[z] = (acc4[:, 256:384] * (inv * (0.125 * LOG2E))).astype(BF16)

    def q_send(i):
        return rcopy(qb.at[z], qb.at[z], s_q.at[i], r_q.at[z], (i * NY + y, tp))

    def q_start(i, _):
        q_send(i).start()
        return 0

    lax.fori_loop(0, z, q_start, 0)
    own_k = (acck[...] * inv).astype(BF16)
    own_v = (accv[...] * inv).astype(BF16)
    wkv[...] = jnp.concatenate([own_k, own_v], axis=1)
    win_send = rcopy(wkv, pwkv, s_w, r_w, ((sp + 1) % (NY * NZ), tp))
    win_send.start()

    query_w = (acc4[:, 384:512] * inv).astype(BF16)
    for load in loads[8:]:
        load.wait()
    rcopy(wkv, pwkv, s_w, r_w, ((sp + NY * NZ - 1) % (NY * NZ), tp)).wait_recv()
    prev = pwkv[...]
    keys = jnp.concatenate([prev[:, :64], own_k], axis=0)
    values = jnp.concatenate([prev[:, 64:], own_v], axis=0)
    q_row, k_col = iota((T, 2 * T), 0), iota((T, 2 * T), 1)
    usable = (k_col > q_row) & (k_col <= q_row + T) & ((k_col >= T) | (sp > 0))
    outs = []
    for h in range(2):
        logit = dot_nt(query_w[:, 64 * h : 64 * h + 64], keys) * (0.125 * LOG2E)
        logit = jnp.where(usable, logit, -jnp.inf)
        sink = sinks[h] * LOG2E
        top = jnp.maximum(jnp.max(logit, axis=1, keepdims=True), sink)
        weight = jnp.exp2(logit - top)
        norm = jnp.sum(weight, axis=1, keepdims=True) + jnp.exp2(sink - top)
        outs.append(dot((weight / norm).astype(BF16), values))
    win_out = jnp.concatenate(outs, axis=1).astype(BF16).astype(F32)
    with_squares(bb, win_out)
    scaled_w = (win_out * wg_v[...]).astype(BF16)
    for n in range(4):
        bb[:, n * 512 : n * 512 + 512] = dot(scaled_w, wo_w[:, n * 512 : n * 512 + 512]).astype(BF16)

    def scatter(buf, dst, ssem, rsem):
        sends = []
        for d in (4, 5, 3, 2, 6, 7, 1):
            to = (tp + d) % NTP
            rows = buf.at[pl.ds(pl.multiple_of(to * 16, 16), 16), :]
            sends.append(rcopy(rows, dst.at[tp], ssem.at[d], rsem.at[tp], (sp, to)))
        for send in sends:
            send.start()
        return sends

    win_sends = scatter(bb, rb, s_rb, r_rb)

    before, after = (y + NY - 2) % NY, (y + 2) % NY
    row_of = lambda d: (z * NY + (y + d) % NY, tp)
    relays = [
        (before, [(kvb.at[before], 1, r_k.at[before]), (kvb.at[before, 0], 2, r_k4.at[0])]),
        (after, [(kvb.at[after], NY - 1, r_k.at[after]), (kvb.at[after, 1], NY - 2, r_k4.at[1])]),
    ]
    for side, (src, copies) in enumerate(relays):
        rcopy(kvb.at[src], kvb.at[src], s_k.at[0], r_k.at[src], row_of(1)).wait_recv()
        for n, (ref, d, rsem) in enumerate(copies):
            send = rcopy(ref, ref, s_k.at[4 + 2 * side + n], rsem, row_of(d))
            send.start()
            kv_sends.append(send)
    for d in (1, 7, 3, 5):
        src = (y + d) % NY
        rcopy(kvb.at[src], kvb.at[src], s_k.at[0], r_k.at[src], row_of(1)).wait_recv()
    far = (y + 4) % NY
    for n in range(2):
        rcopy(kvb.at[far, n], kvb.at[far, n], s_k.at[0], r_k4.at[n], row_of(1)).wait_recv()

    def spread(j, _):
        key_t, val = kvb[j, 0], kvb[j, 1]
        zero = jnp.zeros_like(key_t)
        feat = iota((T, 128), 0) < 64
        kbd[j, :, :T] = jnp.where(feat, key_t, zero)
        kbd[j, :, T:] = jnp.where(feat, zero, key_t)
        lane = iota((T, 128), 1) < 64
        vbd[j, :T, :] = jnp.where(lane, val, zero)
        vbd[j, T:, :] = jnp.where(lane, zero, val)
        return 0

    lax.fori_loop(0, NY, spread, 0)

    bias_row = jnp.where(iota((1, 2 * T), 1) < T, bias[0] * LOG2E, bias[1] * LOG2E)

    def tile(q, j, usable):
        score = dot(q, kbd[j]) + bias_row
        soft = jnp.maximum(score, jnp.log(1.0 + jnp.exp2(jnp.minimum(score, 126.0))) * LOG2E)
        if usable is not None:
            soft = jnp.where(usable, soft, 0.0)
        soft_b = soft.astype(BF16)
        weight = jnp.exp2((score - soft) - dot(soft_b, tri[...]))
        if usable is not None:
            weight = jnp.where(usable, weight, 0.0)
        return dot(weight.astype(BF16), vbd[j]), dot(soft_b, ones[...])

    def log_rows(total):
        flipped = total.T
        return flipped[0:1, :], flipped[64:65, :]

    def p_send(to):
        return rcopy(pout.at[to], prec.at[z], s_p.at[to], r_p.at[z], (to * NY + y, tp))

    def query_step(i, _):
        zq = NZ - 1 - i
        rcopy(qb.at[zq], qb.at[zq], s_q.at[0], r_q.at[zq], (zq * NY + y, tp)).wait_recv()
        q = qb[zq]
        part, logs = tile(q, NY - 1, None)
        for j in range(NY - 2, -1, -1):
            p_j, l_j = tile(q, j, None)
            part = part + jnp.exp2(-logs) * p_j
            logs = logs + l_j
        pout[zq, :T, :] = part.astype(BF16)
        l0, l1 = log_rows(logs)
        h0, h1 = l0.astype(BF16).astype(F32), l1.astype(BF16).astype(F32)
        row = iota((16, 128), 0)
        packed = jnp.where(row == 0, h0, jnp.where(row == 1, l0 - h0, jnp.where(row == 2, h1, l1 - h1)))
        pout[zq, T:, :] = packed.astype(BF16)
        p_send(zq).start()
        return 0

    lax.fori_loop(0, NZ - 1 - z, query_step, 0)

    acc_p[...] = jnp.zeros_like(acc_p)
    acc_l[...] = jnp.zeros_like(acc_l)
    own_q = qb[z]

    def own_step(i, _):
        j = NY - 1 - i
        usable = (j * T + k_col % T) < (y * T + q_row)
        p_j, l_j = tile(own_q, j, usable)
        acc_p[...] += jnp.exp2(-acc_l[...]) * p_j
        acc_l[...] += l_j
        return 0

    lax.fori_loop(NY - 1 - y, NY, own_step, 0)

    def merge(i, logs):
        l0, l1 = logs
        src = z - 1 - i
        rcopy(pout.at[src], prec.at[src], s_p.at[0], r_p.at[src], (src * NY + y, tp)).wait_recv()
        factor = jnp.concatenate(
            [jnp.broadcast_to(jnp.exp2(-l0), (64, 128)), jnp.broadcast_to(jnp.exp2(-l1), (64, 128))], axis=0
        ).T
        acc_p[...] += factor * prec[src, :T, :].astype(F32)
        more = prec[src, T:, :].astype(F32)
        return l0 + (more[0:1] + more[1:2]), l1 + (more[2:3] + more[3:4])

    lax.fori_loop(0, z, merge, log_rows(acc_l[...]))

    stick_out = acc_p[...].astype(BF16).astype(F32)
    with_squares(ab, stick_out)
    scaled_s = (stick_out * sg_v[...]).astype(BF16)
    for n in range(4):
        ab[:, n * 512 : n * 512 + 512] = dot(scaled_s, wo_s[:, n * 512 : n * 512 + 512]).astype(BF16)
    stick_sends = scatter(ab, ra, s_ra, r_ra)

    def gathered(buf, dst, rsem):
        mine = pl.ds(pl.multiple_of(tp * 16, 16), 16)
        total = buf[mine, :].astype(F32)
        for d in (1, 2, 6, 7, 3, 5, 4):
            src = (tp + d) % NTP
            rcopy(dst.at[src], dst.at[src], s_ra.at[0], rsem.at[src], (sp, src)).wait_recv()
            total = total + dst[src].astype(F32)
        scale = lax.rsqrt(jnp.sum(total[:, D:], axis=1, keepdims=True) * (1.0 / 1024) + EPS)
        return total[:, :D] * scale

    combined = gathered(bb, rb, r_rb)
    combined = combined + gathered(ab, ra, r_ra)
    mean = jnp.sum(combined * combined, axis=1, keepdims=True) * (1.0 / D)
    out[...] = (combined * lax.rsqrt(mean + EPS) * post_v[...]).astype(BF16)

    for send in tok_sends + kv_sends + [win_send] + win_sends + stick_sends:
        send.wait_send()
    for n in (4, 5, 6):
        rcopy(own_tok, own_tok, s_a.at[n], r_a.at[tp], (sp, partner)).wait_send()

    def q_drain(i, _):
        q_send(i).wait_send()
        return 0

    lax.fori_loop(0, z, q_drain, 0)

    def p_drain(i, _):
        p_send(NZ - 1 - i).wait_send()
        return 0

    lax.fori_loop(0, NZ - 1 - z, p_drain, 0)


def shards(
    tokens, pre_gain, w_query_stick, w_key_stick, w_value_stick, w_query_window, w_key_window, w_value_window,
    stick_bias, sinks, stick_gain, window_gain, w_out_stick, w_out_window, post_gain,
):
    anywhere = pl.BlockSpec(memory_space=pl.ANY)
    scalars = pl.BlockSpec(memory_space=pltpu.SMEM)
    dma = pltpu.SemaphoreType.DMA
    vm = pltpu.VMEM
    scratch = [
        vm((NTP, T, CH), BF16), vm((D, 512), BF16), vm((D, 64), BF16), vm((D, 64), BF16),
        vm((128, D), BF16), vm((128, D), BF16), vm((1, D), F32), vm((1, 128), F32), vm((1, 128), F32), vm((1, D), F32),
        vm((T, 512), F32), vm((T, 64), F32), vm((T, 64), F32), vm((T, 128), F32),
        vm((NY, 2, T, 128), BF16), vm((NZ, T, 128), BF16), vm((NY, 128, 2 * T), BF16), vm((NY, 2 * T, 128), BF16),
        vm((256, 256), BF16), vm((256, 128), BF16),
        vm((T, 128), BF16), vm((T, 128), BF16), vm((NZ, PROWS, 128), BF16), vm((NZ, PROWS, 128), BF16),
        vm((T, 128), F32), vm((T, 128), F32), vm((T, PACK), BF16), vm((T, PACK), BF16),
        vm((NTP, 16, PACK), BF16), vm((NTP, 16, PACK), BF16),
        dma((13,)), dma((7,)), dma((NTP,)), dma((8,)), dma((NY,)), dma((2,)), dma((NZ,)), dma((NZ,)), dma, dma,
        dma((NZ,)), dma((NZ,)), dma((NTP,)), dma((NTP,)), dma((NTP,)), dma((NTP,)),
    ]
    return pl.pallas_call(
        kernel,
        out_shape=jax.ShapeDtypeStruct((T // NTP, D), BF16),
        in_specs=[anywhere] * 8 + [scalars] * 2 + [anywhere] * 5,
        out_specs=pl.BlockSpec(memory_space=pltpu.VMEM),
        scratch_shapes=scratch,
        compiler_params=pltpu.CompilerParams(
            collective_id=0, has_side_effects=True, vmem_limit_bytes=48 * 1024 * 1024
        ),
    )(
        tokens, pre_gain.reshape(1, -1), w_query_stick, w_key_stick, w_value_stick, w_query_window,
        w_key_window, w_value_window, stick_bias, sinks, stick_gain.reshape(1, -1), window_gain.reshape(1, -1),
        w_out_stick, w_out_window, post_gain.reshape(1, -1),
    )


def solution(mesh):
    in_specs = (
        P("sp", "tp"),
        P(),
        P(None, "tp"),
        P(None, "tp"),
        P(None, "tp"),
        P(None, "tp"),
        P(None, "tp"),
        P(None, "tp"),
        P("tp"),
        P("tp"),
        P("tp"),
        P("tp"),
        P("tp", None),
        P("tp", None),
        P(),
    )
    out_specs = P(("sp", "tp"), None)
    return jax.shard_map(shards, mesh=mesh, in_specs=in_specs, out_specs=out_specs, check_vma=False)
```

```python
import functools

import jax
import jax.numpy as jnp
from jax import lax
from jax.experimental import pallas as pl
from jax.experimental.pallas import tpu as pltpu
from jax.sharding import PartitionSpec as P

T = 128
D = 2048
CH = 256
NY = 8
NZ = 8
NTP = 8
NX = 4
LOG2E = 1.4426950408889634
EPS = 1e-06
PACK = D + 128
PROWS = T + 16
MESH = pl.DeviceIdType.MESH
F32 = jnp.float32
BF16 = jnp.bfloat16


def dot(a, b):
    return jnp.dot(a, b, preferred_element_type=F32)


def dot_nt(a, b):
    return lax.dot_general(a, b, (((1,), (1,)), ((), ())), preferred_element_type=F32)


def iota(shape, dim):
    return lax.broadcasted_iota(jnp.int32, shape, dim)


def with_squares(ref, out):
    total = jnp.sum(out * out, axis=1, keepdims=True)
    high = total.astype(BF16).astype(F32)
    lane = iota((T, 128), 1)
    ref[:, D:] = jnp.where(lane == 0, high, jnp.where(lane == 1, total - high, 0.0)).astype(BF16)


def kernel(
    tok, pre, wqs, wks, wvs, wqw, wkw, wvw, bias, sinks, sgain, wgain, wos, wow, post,
    out,
    tok_all, w4, w_win, wo_s, wo_w, pre_v, sg_v, wg_v, post_v,
    acc4, acc_w, sq, kvb, qb, kbd, vbd, tri, soft_b, diff, weight_b, parts, logs,
    wkv, pwkv, pout, prec, acc_p, ab, bb, ra, rb, bias_s, sinks_s,
    lsem, s_a, r_a, s_k, r_k, r_k4, s_q, r_q, s_w, r_w, ready, s_p, r_p, s_ra, r_ra, s_rb, r_rb,
):
    sp = lax.axis_index("sp")
    tp = lax.axis_index("tp")
    z = sp // NY
    y = sp % NY
    x = tp // 2
    c = tp % 2

    def rcopy(src, dst, ssem, rsem, dev):
        return pltpu.make_async_remote_copy(
            src_ref=src, dst_ref=dst, send_sem=ssem, recv_sem=rsem, device_id=dev, device_id_type=MESH
        )

    loads = [pltpu.make_async_copy(tok, tok_all.at[tp], lsem.at[0])]
    pairs = [
        (pre, pre_v), (wks, w4.at[:, pl.ds(0, 128)]), (wvs, w4.at[:, pl.ds(128, 128)]),
        (wqs, w4.at[:, pl.ds(256, 128)]), (wqw, w4.at[:, pl.ds(384, 128)]),
        (wkw, w_win.at[pl.ds(0, 64), :]), (wvw, w_win.at[pl.ds(64, 64), :]),
        (bias, bias_s), (sinks, sinks_s), (sgain, sg_v), (wgain, wg_v), (post, post_v), (wos, wo_s), (wow, wo_w),
    ]
    for n, (src, dst) in enumerate(pairs):
        loads.append(pltpu.make_async_copy(src, dst, lsem.at[n + 1]))
    for load in loads:
        load.start()

    barrier = pltpu.get_barrier_semaphore()

    def greet(dev):
        pl.semaphore_signal(barrier, inc=1, device_id=dev, device_id_type=MESH)

    greeted = [(sp, (tp + d) % NTP) for d in range(1, NTP)]
    greeted += [(z * NY + (y + d) % NY, tp) for d in (1, 2, NY - 2, NY - 1)]
    for dev in greeted:
        greet(dev)

    def greet_row(i, _):
        greet((i * NY + y, tp))
        return 0

    lax.fori_loop(z + 1, NZ, greet_row, 0)
    has_next = sp < NY * NZ - 1
    has_prev = sp > 0
    starts_row = (y == 0) & has_prev
    ends_row = (y == NY - 1) & has_next
    nxt = ((sp + 1) % (NY * NZ), tp)
    before_me = ((sp + NY * NZ - 1) % (NY * NZ), tp)

    @pl.when(ends_row)
    def _():
        greet(nxt)

    row2, col2 = iota((256, 256), 0), iota((256, 256), 1)
    tri[...] = jnp.where((row2 > col2) & (row2 // T == col2 // T), 1.0, 0.0).astype(BF16)
    acc4[...] = jnp.zeros_like(acc4)
    acc_w[...] = jnp.zeros_like(acc_w)
    sq[...] = jnp.zeros_like(sq)

    pl.semaphore_wait(barrier, len(greeted) + z + jnp.where(starts_row, 1, 0))

    @pl.when(starts_row)
    def _():
        pl.semaphore_signal(ready, inc=1, device_id=before_me, device_id_type=MESH)

    loads[0].wait()

    partner = x * 2 + (1 - c)
    own_tok = tok_all.at[tp]
    tok_sends = []
    for n, d in enumerate((2, 1, 3)):
        peer = ((x + d) % NX) * 2 + c
        tok_sends.append(rcopy(own_tok, own_tok, s_a.at[n], r_a.at[tp], (sp, peer)))
    tok_sends.append(rcopy(own_tok, own_tok, s_a.at[3], r_a.at[tp], (sp, partner)))
    for send in tok_sends:
        send.start()
    for load in loads[1:8]:
        load.wait()

    def feature_step(i, _):
        dist = jnp.where(i < 2, 0, jnp.where((i == 2) | (i == 5), 1, jnp.where((i == 3) | (i == 6), 3, 2)))
        core = jnp.where((i == 1) | (i >= 5), 1 - c, c)
        src = ((x + dist) % NX) * 2 + core
        block = tok_all.at[src]

        @pl.when(i > 0)
        def _():
            rcopy(block, block, s_a.at[0], r_a.at[src], (sp, partner)).wait_recv()

        @pl.when((i >= 2) & (i <= 4))
        def _():
            rcopy(block, block, s_a.at[i + 2], r_a.at[src], (sp, partner)).start()

        feats = block[...].astype(F32)
        sq[...] += feats[:, :128] * feats[:, :128] + feats[:, 128:] * feats[:, 128:]
        at = pl.ds(pl.multiple_of(src * CH, CH), CH)
        scaled = (feats * pre_v[:, at]).astype(BF16)
        acc4[...] += dot(scaled, w4[at, :])
        acc_w[...] += dot_nt(scaled, w_win[:, at])
        return 0

    lax.fori_loop(0, NTP, feature_step, 0)
    inv = lax.rsqrt(jnp.sum(sq[...], axis=1, keepdims=True) * (1.0 / D) + EPS)

    own_pair = (acc_w[...] * inv).astype(BF16)
    wkv[...] = own_pair

    @pl.when(ends_row)
    def _():
        pl.semaphore_wait(ready, 1)

    win_send = rcopy(wkv, pwkv, s_w, r_w, nxt)

    @pl.when(has_next)
    def _():
        win_send.start()

    kvb[y, 0] = (acc4[:, 0:128] * inv).T.astype(BF16)
    kvb[y, 1] = (acc4[:, 128:256] * inv).astype(BF16)
    own_kv = kvb.at[y]
    kv_sends = []
    for n, d in enumerate((2, NY - 2, 1, NY - 1)):
        kv_sends.append(rcopy(own_kv, own_kv, s_k.at[n], r_k.at[y], (z * NY + (y + d) % NY, tp)))
    for send in kv_sends:
        send.start()
    qb[z] = (acc4[:, 256:384] * (inv * (0.125 * LOG2E))).astype(BF16)

    def q_send(i):
        return rcopy(qb.at[z], qb.at[z], s_q.at[i], r_q.at[z], (i * NY + y, tp))

    def q_start(i, _):
        q_send(i).start()
        return 0

    lax.fori_loop(0, z, q_start, 0)

    query_w = (acc4[:, 384:512] * inv).astype(BF16)
    for load in loads[8:]:
        load.wait()

    @pl.when(has_prev)
    def _():
        rcopy(wkv, pwkv, s_w, r_w, before_me).wait_recv()

    @pl.when(jnp.logical_not(has_prev))
    def _():
        pwkv[...] = jnp.zeros_like(pwkv)

    prev = pwkv[...]
    keys = jnp.concatenate([prev[:, :64], own_pair[:, :64]], axis=0)
    values = jnp.concatenate([prev[:, 64:], own_pair[:, 64:]], axis=0)
    q_row, k_col = iota((T, 2 * T), 0), iota((T, 2 * T), 1)
    usable = (k_col > q_row) & (k_col <= q_row + T) & ((k_col >= T) | has_prev)
    outs = []
    for h in range(2):
        logit = dot_nt(query_w[:, 64 * h : 64 * h + 64], keys) * (0.125 * LOG2E)
        logit = jnp.where(usable, logit, -jnp.inf)
        sink = sinks_s[h] * LOG2E
        top = jnp.maximum(jnp.max(logit, axis=1, keepdims=True), sink)
        weight = jnp.exp2(logit - top)
        norm = jnp.sum(weight, axis=1, keepdims=True) + jnp.exp2(sink - top)
        outs.append(dot((weight / norm).astype(BF16), values))
    win_out = jnp.concatenate(outs, axis=1).astype(BF16).astype(F32)
    with_squares(bb, win_out)
    scaled_w = (win_out * wg_v[...]).astype(BF16)
    for n in range(4):
        bb[:, n * 512 : n * 512 + 512] = dot(scaled_w, wo_w[:, n * 512 : n * 512 + 512]).astype(BF16)

    def scatter(buf, dst, ssem, rsem):
        sends = []
        for d in (4, 5, 3, 2, 6, 7, 1):
            to = (tp + d) % NTP
            rows = buf.at[pl.ds(pl.multiple_of(to * 16, 16), 16), :]
            sends.append(rcopy(rows, dst.at[tp], ssem.at[d], rsem.at[tp], (sp, to)))
        for send in sends:
            send.start()
        return sends

    win_sends = scatter(bb, rb, s_rb, r_rb)

    before, after = (y + NY - 2) % NY, (y + 2) % NY
    row_of = lambda d: (z * NY + (y + d) % NY, tp)
    relays = [
        (before, [(kvb.at[before], 1, r_k.at[before]), (kvb.at[before, 0], 2, r_k4.at[0])]),
        (after, [(kvb.at[after], NY - 1, r_k.at[after]), (kvb.at[after, 1], NY - 2, r_k4.at[1])]),
    ]
    for side, (src, copies) in enumerate(relays):
        rcopy(kvb.at[src], kvb.at[src], s_k.at[0], r_k.at[src], row_of(1)).wait_recv()
        for n, (ref, d, rsem) in enumerate(copies):
            send = rcopy(ref, ref, s_k.at[4 + 2 * side + n], rsem, row_of(d))
            send.start()
            kv_sends.append(send)

    def spread(j):
        key_t, val = kvb[j, 0], kvb[j, 1]
        zero = jnp.zeros_like(key_t)
        feat = iota((T, 128), 0) < 64
        kbd[j, :, :T] = jnp.where(feat, key_t, zero)
        kbd[j, :, T:] = jnp.where(feat, zero, key_t)
        lane = iota((T, 128), 1) < 64
        vbd[j, :T, :] = jnp.where(lane, val, zero)
        vbd[j, T:, :] = jnp.where(lane, zero, val)

    bias_row = jnp.where(iota((1, 2 * T), 1) < T, bias_s[0] * LOG2E, bias_s[1] * LOG2E)

    def scores(q, pair, usable_of=None):
        query = qb[q]
        for t, j in enumerate(pair):
            score = dot(query, kbd[j]) + bias_row
            soft = jnp.maximum(score, jnp.log(1.0 + jnp.exp2(jnp.minimum(score, 126.0))) * LOG2E)
            rest = score - soft
            if usable_of is not None:
                usable = usable_of(j)
                soft = jnp.where(usable, soft, 0.0)
                rest = jnp.where(usable, rest, -1e30)
            diff[t] = rest
            soft_b[t] = soft.astype(BF16)
            sum0 = jnp.sum(soft[:, :T], axis=1, keepdims=True)
            sum1 = jnp.sum(soft[:, T:], axis=1, keepdims=True)
            logs[q, j] = jnp.where(iota((T, 128), 1) < 64, sum0, sum1)

    def weights():
        for t in range(2):
            weight_b[t] = jnp.exp2(diff[t] - dot(soft_b[t], tri[...])).astype(BF16)

    def outputs(q, pair):
        for t, j in enumerate(pair):
            parts[q, j] = dot(weight_b[t], vbd[j])

    def visit(pair, first):
        for j in pair:
            spread(j)
        scores(z, pair, lambda j: (j * T + k_col % T) < (y * T + q_row))

        def step(q, _):
            if first:
                rcopy(qb.at[q], qb.at[q], s_q.at[0], r_q.at[q], (q * NY + y, tp)).wait_recv()
            outputs(jnp.where(q - 2 < z, NZ, q - 2), pair)
            weights()
            scores(q, pair)
            return 0

        lax.fori_loop(z + 1, NZ, step, 0)
        outputs(jnp.where(z == NZ - 1, NZ, NZ - 2), pair)
        weights()
        outputs(NZ - 1, pair)

    weight_b[...] = jnp.zeros_like(weight_b)

    def kv_wait(src):
        rcopy(kvb.at[src], kvb.at[src], s_k.at[0], r_k.at[src], row_of(1)).wait_recv()

    far = [(y + d) % NY for d in range(NY)]
    visit((y, before), True)
    kv_wait(far[NY - 1])
    visit((after, far[NY - 1]), False)
    kv_wait(far[1])
    kv_wait(far[NY - 3])
    visit((far[1], far[NY - 3]), False)
    kv_wait(far[3])
    for n in range(2):
        rcopy(kvb.at[far[4], n], kvb.at[far[4], n], s_k.at[0], r_k4.at[n], row_of(1)).wait_recv()
    visit((far[3], far[4]), False)

    def total_of(q):
        part, total = parts[q, NY - 1], logs[q, NY - 1]
        for j in range(NY - 2, -1, -1):
            part = part + jnp.exp2(-total) * parts[q, j]
            total = total + logs[q, j]
        flipped = total.T
        return part, (flipped[0:1, :], flipped[64:65, :])

    def p_send(to):
        return rcopy(pout.at[to], prec.at[z], s_p.at[to], r_p.at[z], (to * NY + y, tp))

    def give(i, _):
        zq = NZ - 1 - i
        part, (l0, l1) = total_of(zq)
        pout[zq, :T, :] = part.astype(BF16)
        h0, h1 = l0.astype(BF16).astype(F32), l1.astype(BF16).astype(F32)
        row = iota((16, 128), 0)
        packed = jnp.where(row == 0, h0, jnp.where(row == 1, l0 - h0, jnp.where(row == 2, h1, l1 - h1)))
        pout[zq, T:, :] = packed.astype(BF16)
        p_send(zq).start()
        return 0

    lax.fori_loop(0, NZ - 1 - z, give, 0)
    own_part, own_logs = total_of(z)
    acc_p[...] = own_part

    def merge(i, rows):
        l0, l1 = rows
        src = z - 1 - i
        rcopy(pout.at[src], prec.at[src], s_p.at[0], r_p.at[src], (src * NY + y, tp)).wait_recv()
        factor = jnp.concatenate(
            [jnp.broadcast_to(jnp.exp2(-l0), (64, 128)), jnp.broadcast_to(jnp.exp2(-l1), (64, 128))], axis=0
        ).T
        acc_p[...] += factor * prec[src, :T, :].astype(F32)
        more = prec[src, T:, :].astype(F32)
        return l0 + (more[0:1] + more[1:2]), l1 + (more[2:3] + more[3:4])

    lax.fori_loop(0, z, merge, own_logs)

    stick_out = acc_p[...].astype(BF16).astype(F32)
    with_squares(ab, stick_out)
    scaled_s = (stick_out * sg_v[...]).astype(BF16)
    for n in range(4):
        ab[:, n * 512 : n * 512 + 512] = dot(scaled_s, wo_s[:, n * 512 : n * 512 + 512]).astype(BF16)
    stick_sends = scatter(ab, ra, s_ra, r_ra)

    def gathered(buf, dst, rsem):
        mine = pl.ds(pl.multiple_of(tp * 16, 16), 16)
        total = buf[mine, :].astype(F32)
        for d in (1, 2, 6, 7, 3, 5, 4):
            src = (tp + d) % NTP
            rcopy(dst.at[src], dst.at[src], s_ra.at[0], rsem.at[src], (sp, src)).wait_recv()
            total = total + dst[src].astype(F32)
        scale = lax.rsqrt(jnp.sum(total[:, D:], axis=1, keepdims=True) * (1.0 / 1024) + EPS)
        return total[:, :D] * scale

    combined = gathered(bb, rb, r_rb)
    combined = combined + gathered(ab, ra, r_ra)
    mean = jnp.sum(combined * combined, axis=1, keepdims=True) * (1.0 / D)
    out[...] = (combined * lax.rsqrt(mean + EPS) * post_v[...]).astype(BF16)

    for send in tok_sends + kv_sends + win_sends + stick_sends:
        send.wait_send()

    @pl.when(has_next)
    def _():
        win_send.wait_send()

    for n in (4, 5, 6):
        rcopy(own_tok, own_tok, s_a.at[n], r_a.at[tp], (sp, partner)).wait_send()

    def q_drain(i, _):
        q_send(i).wait_send()
        return 0

    lax.fori_loop(0, z, q_drain, 0)

    def p_drain(i, _):
        p_send(NZ - 1 - i).wait_send()
        return 0

    lax.fori_loop(0, NZ - 1 - z, p_drain, 0)


def shards(
    tokens, pre_gain, w_query_stick, w_key_stick, w_value_stick, w_query_window, w_key_window, w_value_window,
    stick_bias, sinks, stick_gain, window_gain, w_out_stick, w_out_window, post_gain,
):
    anywhere = pl.BlockSpec(memory_space=pl.ANY)
    dma = pltpu.SemaphoreType.DMA
    vm = pltpu.VMEM
    scratch = [
        vm((NTP, T, CH), BF16), vm((D, 512), BF16), vm((128, D), BF16),
        vm((128, D), BF16), vm((128, D), BF16), vm((1, D), F32), vm((1, 128), F32), vm((1, 128), F32), vm((1, D), F32),
        vm((T, 512), F32), vm((T, 128), F32), vm((T, 128), F32),
        vm((NY, 2, T, 128), BF16), vm((NZ, T, 128), BF16), vm((NY, 128, 2 * T), BF16), vm((NY, 2 * T, 128), BF16),
        vm((256, 256), BF16), vm((2, T, 2 * T), BF16), vm((2, T, 2 * T), F32), vm((2, T, 2 * T), BF16),
        vm((NZ + 1, NY, T, 128), F32), vm((NZ + 1, NY, T, 128), F32),
        vm((T, 128), BF16), vm((T, 128), BF16), vm((NZ, PROWS, 128), BF16), vm((NZ, PROWS, 128), BF16),
        vm((T, 128), F32), vm((T, PACK), BF16), vm((T, PACK), BF16),
        vm((NTP, 16, PACK), BF16), vm((NTP, 16, PACK), BF16), pltpu.SMEM((2,), F32), pltpu.SMEM((2,), F32),
        dma((15,)), dma((7,)), dma((NTP,)), dma((8,)), dma((NY,)), dma((2,)), dma((NZ,)), dma((NZ,)), dma, dma, pltpu.SemaphoreType.REGULAR,
        dma((NZ,)), dma((NZ,)), dma((NTP,)), dma((NTP,)), dma((NTP,)), dma((NTP,)),
    ]
    return pl.pallas_call(
        kernel,
        out_shape=jax.ShapeDtypeStruct((T // NTP, D), BF16),
        in_specs=[anywhere] * 15,
        out_specs=pl.BlockSpec(memory_space=pltpu.VMEM),
        scratch_shapes=scratch,
        compiler_params=pltpu.CompilerParams(
            collective_id=0, has_side_effects=True, vmem_limit_bytes=60 * 1024 * 1024
        ),
    )(
        tokens, pre_gain.reshape(1, -1), w_query_stick, w_key_stick, w_value_stick, w_query_window,
        w_key_window.T, w_value_window.T, stick_bias, sinks, stick_gain.reshape(1, -1), window_gain.reshape(1, -1),
        w_out_stick, w_out_window, post_gain.reshape(1, -1),
    )


def solution(mesh):
    in_specs = (
        P("sp", "tp"),
        P(),
        P(None, "tp"),
        P(None, "tp"),
        P(None, "tp"),
        P(None, "tp"),
        P(None, "tp"),
        P(None, "tp"),
        P("tp"),
        P("tp"),
        P("tp"),
        P("tp"),
        P("tp", None),
        P("tp", None),
        P(),
    )
    out_specs = P(("sp", "tp"), None)
    return jax.shard_map(shards, mesh=mesh, in_specs=in_specs, out_specs=out_specs, check_vma=False)
```

```python
import functools

import jax
import jax.numpy as jnp
from jax import lax
from jax.experimental import pallas as pl
from jax.experimental.pallas import tpu as pltpu
from jax.sharding import PartitionSpec as P

T = 128
D = 2048
CH = 256
NY = 8
NZ = 8
NTP = 8
NX = 4
LOG2E = 1.4426950408889634
EPS = 1e-06
PACK = D + 128
PROWS = T + 16
MESH = pl.DeviceIdType.MESH
F32 = jnp.float32
BF16 = jnp.bfloat16


def dot(a, b):
    return jnp.dot(a, b, preferred_element_type=F32)


def dot_nt(a, b):
    return lax.dot_general(a, b, (((1,), (1,)), ((), ())), preferred_element_type=F32)


def iota(shape, dim):
    return lax.broadcasted_iota(jnp.int32, shape, dim)


def with_squares(ref, out):
    total = jnp.sum(out * out, axis=1, keepdims=True)
    high = total.astype(BF16).astype(F32)
    lane = iota((T, 128), 1)
    ref[:, D:] = jnp.where(lane == 0, high, jnp.where(lane == 1, total - high, 0.0)).astype(BF16)


def kernel(
    tok, pre, wqs, wks, wvs, wqw, wkw, wvw, bias, sinks, sgain, wgain, wos, wow, post,
    out,
    tok_all, w4, w_win, wo_s, wo_w, pre_v, sg_v, wg_v, post_v,
    acc4, acc_w, sq, kvb, qb, kbd, vbd, tri, raw, soft_b, diff, expo, weight_b, parts, logs,
    wkv, pwkv, pout, prec, acc_p, ab, bb, ra, rb, bias_s, sinks_s,
    lsem, s_a, r_a, s_k, r_k, r_k4, s_q, r_q, s_w, r_w, ready, s_p, r_p, s_ra, r_ra, s_rb, r_rb,
):
    sp = lax.axis_index("sp")
    tp = lax.axis_index("tp")
    z = sp // NY
    y = sp % NY
    x = tp // 2
    c = tp % 2

    def rcopy(src, dst, ssem, rsem, dev):
        return pltpu.make_async_remote_copy(
            src_ref=src, dst_ref=dst, send_sem=ssem, recv_sem=rsem, device_id=dev, device_id_type=MESH
        )

    def rows_of(block, count=1):
        return pl.ds(pl.multiple_of(block * T, T), count * T)

    loads = [pltpu.make_async_copy(tok, tok_all.at[tp], lsem.at[0])]
    pairs = [
        (pre, pre_v), (wks, w4.at[:, pl.ds(0, 128)]), (wvs, w4.at[:, pl.ds(128, 128)]),
        (wqs, w4.at[:, pl.ds(256, 128)]), (wqw, w4.at[:, pl.ds(384, 128)]),
        (wkw, w_win.at[pl.ds(0, 64), :]), (wvw, w_win.at[pl.ds(64, 64), :]),
        (bias, bias_s), (sinks, sinks_s), (sgain, sg_v), (wgain, wg_v), (post, post_v), (wos, wo_s), (wow, wo_w),
    ]
    for n, (src, dst) in enumerate(pairs):
        loads.append(pltpu.make_async_copy(src, dst, lsem.at[n + 1]))
    for load in loads:
        load.start()

    barrier = pltpu.get_barrier_semaphore()

    def greet(dev):
        pl.semaphore_signal(barrier, inc=1, device_id=dev, device_id_type=MESH)

    greeted = [(sp, (tp + d) % NTP) for d in range(1, NTP)]
    greeted += [(z * NY + (y + d) % NY, tp) for d in (1, 2, NY - 2, NY - 1)]
    for dev in greeted:
        greet(dev)

    def greet_row(i, _):
        greet((i * NY + y, tp))
        return 0

    lax.fori_loop(z + 1, NZ, greet_row, 0)
    has_next = sp < NY * NZ - 1
    has_prev = sp > 0
    starts_row = (y == 0) & has_prev
    ends_row = (y == NY - 1) & has_next
    nxt = ((sp + 1) % (NY * NZ), tp)
    before_me = ((sp + NY * NZ - 1) % (NY * NZ), tp)

    @pl.when(ends_row)
    def _():
        greet(nxt)

    row2, col2 = iota((256, 256), 0), iota((256, 256), 1)
    tri[...] = jnp.where((row2 > col2) & (row2 // T == col2 // T), 1.0, 0.0).astype(BF16)
    acc4[...] = jnp.zeros_like(acc4)
    acc_w[...] = jnp.zeros_like(acc_w)
    sq[...] = jnp.zeros_like(sq)
    for ref in (raw, soft_b, diff, expo, weight_b):
        ref[...] = jnp.zeros_like(ref)
    qb[NZ * T :, :] = jnp.zeros((T, 128), BF16)

    pl.semaphore_wait(barrier, len(greeted) + z + jnp.where(starts_row, 1, 0))

    @pl.when(starts_row)
    def _():
        pl.semaphore_signal(ready, inc=1, device_id=before_me, device_id_type=MESH)

    loads[0].wait()

    partner = x * 2 + (1 - c)
    own_tok = tok_all.at[tp]
    tok_sends = []
    for n, d in enumerate((2, 1, 3)):
        peer = ((x + d) % NX) * 2 + c
        tok_sends.append(rcopy(own_tok, own_tok, s_a.at[n], r_a.at[tp], (sp, peer)))
    tok_sends.append(rcopy(own_tok, own_tok, s_a.at[3], r_a.at[tp], (sp, partner)))
    for send in tok_sends:
        send.start()
    for load in loads[1:8]:
        load.wait()

    def feature_step(i, _):
        dist = jnp.where(i < 2, 0, jnp.where((i == 2) | (i == 5), 1, jnp.where((i == 3) | (i == 6), 3, 2)))
        core = jnp.where((i == 1) | (i >= 5), 1 - c, c)
        src = ((x + dist) % NX) * 2 + core
        block = tok_all.at[src]

        @pl.when(i > 0)
        def _():
            rcopy(block, block, s_a.at[0], r_a.at[src], (sp, partner)).wait_recv()

        @pl.when((i >= 2) & (i <= 4))
        def _():
            rcopy(block, block, s_a.at[i + 2], r_a.at[src], (sp, partner)).start()

        feats = block[...].astype(F32)
        sq[...] += feats[:, :128] * feats[:, :128] + feats[:, 128:] * feats[:, 128:]
        at = pl.ds(pl.multiple_of(src * CH, CH), CH)
        scaled = (feats * pre_v[:, at]).astype(BF16)
        acc4[...] += dot(scaled, w4[at, :])
        acc_w[...] += dot_nt(scaled, w_win[:, at])
        return 0

    lax.fori_loop(0, NTP, feature_step, 0)
    inv = lax.rsqrt(jnp.sum(sq[...], axis=1, keepdims=True) * (1.0 / D) + EPS)

    own_pair = (acc_w[...] * inv).astype(BF16)
    wkv[...] = own_pair

    @pl.when(ends_row)
    def _():
        pl.semaphore_wait(ready, 1)

    win_send = rcopy(wkv, pwkv, s_w, r_w, nxt)

    @pl.when(has_next)
    def _():
        win_send.start()

    kvb[y, 0] = (acc4[:, 0:128] * inv).T.astype(BF16)
    kvb[y, 1] = (acc4[:, 128:256] * inv).astype(BF16)
    own_kv = kvb.at[y]
    kv_sends = []
    for n, d in enumerate((2, NY - 2, 1, NY - 1)):
        kv_sends.append(rcopy(own_kv, own_kv, s_k.at[n], r_k.at[y], (z * NY + (y + d) % NY, tp)))
    for send in kv_sends:
        send.start()
    qb[rows_of(z), :] = (acc4[:, 256:384] * (inv * (0.125 * LOG2E))).astype(BF16)

    def q_send(i):
        return rcopy(qb.at[rows_of(z), :], qb.at[rows_of(z), :], s_q.at[i], r_q.at[z], (i * NY + y, tp))

    def q_start(i, _):
        q_send(i).start()
        return 0

    lax.fori_loop(0, z, q_start, 0)

    query_w = (acc4[:, 384:512] * inv).astype(BF16)
    for load in loads[8:]:
        load.wait()

    @pl.when(has_prev)
    def _():
        rcopy(wkv, pwkv, s_w, r_w, before_me).wait_recv()

    @pl.when(jnp.logical_not(has_prev))
    def _():
        pwkv[...] = jnp.zeros_like(pwkv)

    prev = pwkv[...]
    keys = jnp.concatenate([prev[:, :64], own_pair[:, :64]], axis=0)
    values = jnp.concatenate([prev[:, 64:], own_pair[:, 64:]], axis=0)
    q_row, k_col = iota((T, 2 * T), 0), iota((T, 2 * T), 1)
    usable = (k_col > q_row) & (k_col <= q_row + T) & ((k_col >= T) | has_prev)
    outs = []
    for h in range(2):
        logit = dot_nt(query_w[:, 64 * h : 64 * h + 64], keys) * (0.125 * LOG2E)
        logit = jnp.where(usable, logit, -jnp.inf)
        sink = sinks_s[h] * LOG2E
        top = jnp.maximum(jnp.max(logit, axis=1, keepdims=True), sink)
        weight = jnp.exp2(logit - top)
        norm = jnp.sum(weight, axis=1, keepdims=True) + jnp.exp2(sink - top)
        outs.append(dot((weight / norm).astype(BF16), values))
    win_out = jnp.concatenate(outs, axis=1).astype(BF16).astype(F32)
    with_squares(bb, win_out)
    scaled_w = (win_out * wg_v[...]).astype(BF16)
    for n in range(4):
        bb[:, n * 512 : n * 512 + 512] = dot(scaled_w, wo_w[:, n * 512 : n * 512 + 512]).astype(BF16)

    def scatter(buf, dst, ssem, rsem):
        sends = []
        for d in (4, 5, 3, 2, 6, 7, 1):
            to = (tp + d) % NTP
            rows = buf.at[pl.ds(pl.multiple_of(to * 16, 16), 16), :]
            sends.append(rcopy(rows, dst.at[tp], ssem.at[d], rsem.at[tp], (sp, to)))
        for send in sends:
            send.start()
        return sends

    win_sends = scatter(bb, rb, s_rb, r_rb)

    before, after = (y + NY - 2) % NY, (y + 2) % NY
    row_of = lambda d: (z * NY + (y + d) % NY, tp)
    relays = [
        (before, [(kvb.at[before], 1, r_k.at[before]), (kvb.at[before, 0], 2, r_k4.at[0])]),
        (after, [(kvb.at[after], NY - 1, r_k.at[after]), (kvb.at[after, 1], NY - 2, r_k4.at[1])]),
    ]
    for side, (src, copies) in enumerate(relays):
        rcopy(kvb.at[src], kvb.at[src], s_k.at[0], r_k.at[src], row_of(1)).wait_recv()
        for n, (ref, d, rsem) in enumerate(copies):
            send = rcopy(ref, ref, s_k.at[4 + 2 * side + n], rsem, row_of(d))
            send.start()
            kv_sends.append(send)

    def spread(j):
        key_t, val = kvb[j, 0], kvb[j, 1]
        zero = jnp.zeros_like(key_t)
        feat = iota((T, 128), 0) < 64
        kbd[j, :, :T] = jnp.where(feat, key_t, zero)
        kbd[j, :, T:] = jnp.where(feat, zero, key_t)
        lane = iota((T, 128), 1) < 64
        vbd[j, :T, :] = jnp.where(lane, val, zero)
        vbd[j, T:, :] = jnp.where(lane, zero, val)

    bias_row = jnp.where(iota((1, 2 * T), 1) < T, bias_s[0] * LOG2E, bias_s[1] * LOG2E)

    in_head0 = iota((2 * T, 128), 1) < 64
    far = [(y + d) % NY for d in range(NY)]
    query_pairs = (NZ - z + 1) // 2
    early = jnp.minimum(query_pairs, 2)
    late = query_pairs - early
    units = 4 * query_pairs

    def unit(i):
        at = jnp.clip(i, 0, units - 1)
        rest = jnp.maximum(at - 3 * early, 0)
        width = jnp.maximum(late, 1)
        in_early, in_last = at < 3 * early, at >= 3 * query_pairs
        k = jnp.where(in_early, at // early, jnp.where(in_last, 3, rest // width))
        p = jnp.where(in_early, at % early, jnp.where(in_last, at - 3 * query_pairs, early + rest % width))
        first = jnp.where(k == 0, y, jnp.where(k == 1, after, jnp.where(k == 2, far[1], far[3])))
        second = jnp.where(k == 0, before, jnp.where(k == 1, far[7], jnp.where(k == 2, far[5], far[4])))
        rows = rows_of(jnp.where((i >= 0) & (i < units), z + 2 * p, NZ + 1), 2)
        return p, (first, second), rows

    halves = (pl.ds(0, 2 * T), pl.ds(2 * T, 2 * T))

    def kv_wait(src):
        rcopy(kvb.at[src], kvb.at[src], s_k.at[0], r_k.at[src], row_of(1)).wait_recv()

    def await_queries(p):
        for n in range(2):
            q = z + 2 * p + n

            @pl.when((q > z) & (q < NZ))
            def _(q=q):
                block = qb.at[rows_of(q), :]
                rcopy(block, block, s_q.at[0], r_q.at[q], (q * NY + y, tp)).wait_recv()

    def unit_step(i, _):
        p, pair, rows = unit(i)

        @pl.when((i < early) | ((i >= 3 * early) & (i < 3 * early + late)))
        def _():
            await_queries(p)

        @pl.when(i == early)
        def _():
            kv_wait(far[7])
            spread(far[7])

        @pl.when(i == 2 * early)
        def _():
            for d in (1, 5):
                kv_wait(far[d])
                spread(far[d])

        @pl.when(i == 3 * query_pairs)
        def _():
            kv_wait(far[3])
            spread(far[3])
            for n in range(2):
                rcopy(kvb.at[far[4], n], kvb.at[far[4], n], s_k.at[0], r_k4.at[n], row_of(1)).wait_recv()
            spread(far[4])

        _, pair_d, rows_d = unit(i - 4)
        for half, j in zip(halves, pair_d):
            parts[j, rows_d, :] = dot(weight_b[half, :], vbd[j])
        weight_b[...] = jnp.exp2(expo[...]).astype(BF16)
        expo[...] = diff[...] - dot(soft_b[...], tri[...])
        _, pair_b, rows_b = unit(i - 1)
        for half, j in zip(halves, pair_b):
            score = raw[half, :] + bias_row
            soft = jnp.maximum(score, jnp.log(1.0 + jnp.exp2(jnp.minimum(score, 126.0))) * LOG2E)
            diff[half, :] = score - soft
            soft_b[half, :] = soft.astype(BF16)
            sum0 = jnp.sum(soft[:, :T], axis=1, keepdims=True)
            sum1 = jnp.sum(soft[:, T:], axis=1, keepdims=True)
            logs[j, rows_b, :] = jnp.where(in_head0, sum0, sum1)
        own_rows = rows_of(jnp.minimum(z + 2 * p, NZ - 1), 2)
        for half, j in zip(halves, pair):
            raw[half, :] = dot(qb[own_rows, :], kbd[j])

        @pl.when(p == 0)
        def _():
            for n, j in enumerate(pair):
                mine = pl.ds(2 * T * n, T)
                raw[mine, :] = jnp.where(k_col % T - q_row < (y - j) * T, raw[mine, :], -1e30)

        return 0

    spread(y)
    spread(before)
    spread(after)
    lax.fori_loop(0, units + 4, unit_step, 0)

    def total_of(q):
        rows = rows_of(q)
        part, total = parts[NY - 1, rows, :], logs[NY - 1, rows, :]
        for j in range(NY - 2, -1, -1):
            part = part + jnp.exp2(-total) * parts[j, rows, :]
            total = total + logs[j, rows, :]
        flipped = total.T
        return part, (flipped[0:1, :], flipped[64:65, :])

    def p_send(to):
        return rcopy(pout.at[to], prec.at[z], s_p.at[to], r_p.at[z], (to * NY + y, tp))

    def give(i, _):
        zq = NZ - 1 - i
        part, (l0, l1) = total_of(zq)
        pout[zq, :T, :] = part.astype(BF16)
        h0, h1 = l0.astype(BF16).astype(F32), l1.astype(BF16).astype(F32)
        row = iota((16, 128), 0)
        packed = jnp.where(row == 0, h0, jnp.where(row == 1, l0 - h0, jnp.where(row == 2, h1, l1 - h1)))
        pout[zq, T:, :] = packed.astype(BF16)
        p_send(zq).start()
        return 0

    lax.fori_loop(0, NZ - 1 - z, give, 0)
    own_part, own_logs = total_of(z)
    acc_p[...] = own_part

    def merge(i, rows):
        l0, l1 = rows
        src = z - 1 - i
        rcopy(pout.at[src], prec.at[src], s_p.at[0], r_p.at[src], (src * NY + y, tp)).wait_recv()
        factor = jnp.concatenate(
            [jnp.broadcast_to(jnp.exp2(-l0), (64, 128)), jnp.broadcast_to(jnp.exp2(-l1), (64, 128))], axis=0
        ).T
        acc_p[...] += factor * prec[src, :T, :].astype(F32)
        more = prec[src, T:, :].astype(F32)
        return l0 + (more[0:1] + more[1:2]), l1 + (more[2:3] + more[3:4])

    lax.fori_loop(0, z, merge, own_logs)

    stick_out = acc_p[...].astype(BF16).astype(F32)
    with_squares(ab, stick_out)
    scaled_s = (stick_out * sg_v[...]).astype(BF16)
    for n in range(4):
        ab[:, n * 512 : n * 512 + 512] = dot(scaled_s, wo_s[:, n * 512 : n * 512 + 512]).astype(BF16)
    stick_sends = scatter(ab, ra, s_ra, r_ra)

    def gathered(buf, dst, rsem):
        mine = pl.ds(pl.multiple_of(tp * 16, 16), 16)
        total = buf[mine, :].astype(F32)
        for d in (1, 2, 6, 7, 3, 5, 4):
            src = (tp + d) % NTP
            rcopy(dst.at[src], dst.at[src], s_ra.at[0], rsem.at[src], (sp, src)).wait_recv()
            total = total + dst[src].astype(F32)
        scale = lax.rsqrt(jnp.sum(total[:, D:], axis=1, keepdims=True) * (1.0 / 1024) + EPS)
        return total[:, :D] * scale

    combined = gathered(bb, rb, r_rb)
    combined = combined + gathered(ab, ra, r_ra)
    mean = jnp.sum(combined * combined, axis=1, keepdims=True) * (1.0 / D)
    out[...] = (combined * lax.rsqrt(mean + EPS) * post_v[...]).astype(BF16)

    for send in tok_sends + kv_sends + win_sends + stick_sends:
        send.wait_send()

    @pl.when(has_next)
    def _():
        win_send.wait_send()

    for n in (4, 5, 6):
        rcopy(own_tok, own_tok, s_a.at[n], r_a.at[tp], (sp, partner)).wait_send()

    def q_drain(i, _):
        q_send(i).wait_send()
        return 0

    lax.fori_loop(0, z, q_drain, 0)

    def p_drain(i, _):
        p_send(NZ - 1 - i).wait_send()
        return 0

    lax.fori_loop(0, NZ - 1 - z, p_drain, 0)


def shards(
    tokens, pre_gain, w_query_stick, w_key_stick, w_value_stick, w_query_window, w_key_window, w_value_window,
    stick_bias, sinks, stick_gain, window_gain, w_out_stick, w_out_window, post_gain,
):
    anywhere = pl.BlockSpec(memory_space=pl.ANY)
    dma = pltpu.SemaphoreType.DMA
    vm = pltpu.VMEM
    scratch = [
        vm((NTP, T, CH), BF16), vm((D, 512), BF16), vm((128, D), BF16),
        vm((128, D), BF16), vm((128, D), BF16), vm((1, D), F32), vm((1, 128), F32), vm((1, 128), F32), vm((1, D), F32),
        vm((T, 512), F32), vm((T, 128), F32), vm((T, 128), F32),
        vm((NY, 2, T, 128), BF16), vm(((NZ + 1) * T, 128), BF16), vm((NY, 128, 2 * T), BF16), vm((NY, 2 * T, 128), BF16),
        vm((256, 256), BF16), vm((4 * T, 2 * T), F32), vm((4 * T, 2 * T), BF16), vm((4 * T, 2 * T), F32), vm((4 * T, 2 * T), F32),
        vm((4 * T, 2 * T), BF16),
        vm((NY, (NZ + 3) * T, 128), F32), vm((NY, (NZ + 3) * T, 128), F32),
        vm((T, 128), BF16), vm((T, 128), BF16), vm((NZ, PROWS, 128), BF16), vm((NZ, PROWS, 128), BF16),
        vm((T, 128), F32), vm((T, PACK), BF16), vm((T, PACK), BF16),
        vm((NTP, 16, PACK), BF16), vm((NTP, 16, PACK), BF16), pltpu.SMEM((2,), F32), pltpu.SMEM((2,), F32),
        dma((15,)), dma((7,)), dma((NTP,)), dma((8,)), dma((NY,)), dma((2,)), dma((NZ,)), dma((NZ,)), dma, dma, pltpu.SemaphoreType.REGULAR,
        dma((NZ,)), dma((NZ,)), dma((NTP,)), dma((NTP,)), dma((NTP,)), dma((NTP,)),
    ]
    return pl.pallas_call(
        kernel,
        out_shape=jax.ShapeDtypeStruct((T // NTP, D), BF16),
        in_specs=[anywhere] * 15,
        out_specs=pl.BlockSpec(memory_space=pltpu.VMEM),
        scratch_shapes=scratch,
        compiler_params=pltpu.CompilerParams(
            collective_id=0, has_side_effects=True, vmem_limit_bytes=60 * 1024 * 1024
        ),
    )(
        tokens, pre_gain.reshape(1, -1), w_query_stick, w_key_stick, w_value_stick, w_query_window,
        w_key_window.T, w_value_window.T, stick_bias, sinks, stick_gain.reshape(1, -1), window_gain.reshape(1, -1),
        w_out_stick, w_out_window, post_gain.reshape(1, -1),
    )


def solution(mesh):
    in_specs = (
        P("sp", "tp"),
        P(),
        P(None, "tp"),
        P(None, "tp"),
        P(None, "tp"),
        P(None, "tp"),
        P(None, "tp"),
        P(None, "tp"),
        P("tp"),
        P("tp"),
        P("tp"),
        P("tp"),
        P("tp", None),
        P("tp", None),
        P(),
    )
    out_specs = P(("sp", "tp"), None)
    return jax.shard_map(shards, mesh=mesh, in_specs=in_specs, out_specs=out_specs, check_vma=False)
```

```python
import functools

import jax
import jax.numpy as jnp
from jax import lax
from jax.experimental import pallas as pl
from jax.experimental.pallas import tpu as pltpu
from jax.sharding import PartitionSpec as P

T = 128
D = 2048
CH = 256
NY = 8
NZ = 8
NTP = 8
NX = 4
LOG2E = 1.4426950408889634
EPS = 1e-06
PACK = D + 128
PROWS = T + 16
MESH = pl.DeviceIdType.MESH
F32 = jnp.float32
BF16 = jnp.bfloat16


def dot(a, b):
    return jnp.dot(a, b, preferred_element_type=F32)


def dot_nt(a, b):
    return lax.dot_general(a, b, (((1,), (1,)), ((), ())), preferred_element_type=F32)


def iota(shape, dim):
    return lax.broadcasted_iota(jnp.int32, shape, dim)


def with_squares(ref, out):
    total = jnp.sum(out * out, axis=1, keepdims=True)
    high = total.astype(BF16).astype(F32)
    lane = iota((T, 128), 1)
    ref[:, D:] = jnp.where(lane == 0, high, jnp.where(lane == 1, total - high, 0.0)).astype(BF16)


def kernel(
    tok, pre, wqs, wks, wvs, wqw, wkw, wvw, bias, sinks, sgain, wgain, wos, wow, post,
    out,
    tok_all, w4, w_win, wo_s, wo_w, pre_v, sg_v, wg_v, post_v,
    acc4, acc_w, sq, kvb, qb, kbd, vbd, tri, raw, soft_b, diff, expo, weight_b, parts, logs, offset,
    wkv, pwkv, pout, prec, acc_p, ab, bb, ra, rb, bias_s, sinks_s,
    lsem, s_a, r_a, s_k, r_k, r_k4, s_q, r_q, s_w, r_w, ready, s_p, r_p, s_ra, r_ra, s_rb, r_rb,
):
    sp = lax.axis_index("sp")
    tp = lax.axis_index("tp")
    z = sp // NY
    y = sp % NY
    x = tp // 2
    c = tp % 2

    def rcopy(src, dst, ssem, rsem, dev):
        return pltpu.make_async_remote_copy(
            src_ref=src, dst_ref=dst, send_sem=ssem, recv_sem=rsem, device_id=dev, device_id_type=MESH
        )

    def rows_of(block, count=1):
        return pl.ds(pl.multiple_of(block * T, T), count * T)

    loads = [pltpu.make_async_copy(tok, tok_all.at[tp], lsem.at[0])]
    pairs = [
        (pre, pre_v), (wks, w4.at[:, pl.ds(0, 128)]), (wvs, w4.at[:, pl.ds(128, 128)]),
        (wqs, w4.at[:, pl.ds(256, 128)]), (wqw, w4.at[:, pl.ds(384, 128)]),
        (wkw, w_win.at[pl.ds(0, 64), :]), (wvw, w_win.at[pl.ds(64, 64), :]),
        (bias, bias_s), (sinks, sinks_s), (sgain, sg_v), (wgain, wg_v), (post, post_v), (wos, wo_s), (wow, wo_w),
    ]
    for n, (src, dst) in enumerate(pairs):
        loads.append(pltpu.make_async_copy(src, dst, lsem.at[n + 1]))
    for load in loads:
        load.start()

    barrier = pltpu.get_barrier_semaphore()

    def greet(dev):
        pl.semaphore_signal(barrier, inc=1, device_id=dev, device_id_type=MESH)

    greeted = [(sp, (tp + d) % NTP) for d in range(1, NTP)]
    greeted += [(z * NY + (y + d) % NY, tp) for d in (1, 2, NY - 2, NY - 1)]
    for dev in greeted:
        greet(dev)

    def greet_row(i, _):
        greet((i * NY + y, tp))
        return 0

    lax.fori_loop(z + 1, NZ, greet_row, 0)
    has_next = sp < NY * NZ - 1
    has_prev = sp > 0
    starts_row = (y == 0) & has_prev
    ends_row = (y == NY - 1) & has_next
    nxt = ((sp + 1) % (NY * NZ), tp)
    before_me = ((sp + NY * NZ - 1) % (NY * NZ), tp)

    @pl.when(ends_row)
    def _():
        greet(nxt)

    row2, col2 = iota((256, 256), 0), iota((256, 256), 1)
    tri[...] = jnp.where((row2 > col2) & (row2 // T == col2 // T), 1.0, 0.0).astype(BF16)
    offset[...] = iota((T, 2 * T), 1) % T - iota((T, 2 * T), 0)
    acc4[...] = jnp.zeros_like(acc4)
    acc_w[...] = jnp.zeros_like(acc_w)
    sq[...] = jnp.zeros_like(sq)
    for ref in (raw, soft_b, diff, expo, weight_b):
        ref[...] = jnp.zeros_like(ref)
    qb[NZ * T :, :] = jnp.zeros((T, 128), BF16)

    pl.semaphore_wait(barrier, len(greeted) + z + jnp.where(starts_row, 1, 0))

    @pl.when(starts_row)
    def _():
        pl.semaphore_signal(ready, inc=1, device_id=before_me, device_id_type=MESH)

    loads[0].wait()

    partner = x * 2 + (1 - c)
    own_tok = tok_all.at[tp]
    tok_sends = []
    for n, d in enumerate((2, 1, 3)):
        peer = ((x + d) % NX) * 2 + c
        tok_sends.append(rcopy(own_tok, own_tok, s_a.at[n], r_a.at[tp], (sp, peer)))
    tok_sends.append(rcopy(own_tok, own_tok, s_a.at[3], r_a.at[tp], (sp, partner)))
    for send in tok_sends:
        send.start()
    for load in loads[1:8]:
        load.wait()

    def feature_step(i, _):
        dist = jnp.where(i < 2, 0, jnp.where((i == 2) | (i == 5), 1, jnp.where((i == 3) | (i == 6), 3, 2)))
        core = jnp.where((i == 1) | (i >= 5), 1 - c, c)
        src = ((x + dist) % NX) * 2 + core
        block = tok_all.at[src]

        @pl.when(i > 0)
        def _():
            rcopy(block, block, s_a.at[0], r_a.at[src], (sp, partner)).wait_recv()

        @pl.when((i >= 2) & (i <= 4))
        def _():
            rcopy(block, block, s_a.at[i + 2], r_a.at[src], (sp, partner)).start()

        feats = block[...].astype(F32)
        sq[...] += feats[:, :128] * feats[:, :128] + feats[:, 128:] * feats[:, 128:]
        at = pl.ds(pl.multiple_of(src * CH, CH), CH)
        scaled = (feats * pre_v[:, at]).astype(BF16)
        acc4[...] += dot(scaled, w4[at, :])
        acc_w[...] += dot_nt(scaled, w_win[:, at])
        return 0

    lax.fori_loop(0, NTP, feature_step, 0)
    inv = lax.rsqrt(jnp.sum(sq[...], axis=1, keepdims=True) * (1.0 / D) + EPS)

    own_pair = (acc_w[...] * inv).astype(BF16)
    wkv[...] = own_pair

    @pl.when(ends_row)
    def _():
        pl.semaphore_wait(ready, 1)

    win_send = rcopy(wkv, pwkv, s_w, r_w, nxt)

    @pl.when(has_next)
    def _():
        win_send.start()

    kvb[y, 0] = (acc4[:, 0:128] * inv).T.astype(BF16)
    kvb[y, 1] = (acc4[:, 128:256] * inv).astype(BF16)
    own_kv = kvb.at[y]
    kv_sends = []
    for n, d in enumerate((2, NY - 2, 1, NY - 1)):
        kv_sends.append(rcopy(own_kv, own_kv, s_k.at[n], r_k.at[y], (z * NY + (y + d) % NY, tp)))
    for send in kv_sends:
        send.start()
    qb[rows_of(z), :] = (acc4[:, 256:384] * (inv * (0.125 * LOG2E))).astype(BF16)

    def q_send(i):
        return rcopy(qb.at[rows_of(z), :], qb.at[rows_of(z), :], s_q.at[i], r_q.at[z], (i * NY + y, tp))

    def q_start(i, _):
        q_send(i).start()
        return 0

    lax.fori_loop(0, z, q_start, 0)

    query_w = (acc4[:, 384:512] * inv).astype(BF16)
    for load in loads[8:]:
        load.wait()

    @pl.when(has_prev)
    def _():
        rcopy(wkv, pwkv, s_w, r_w, before_me).wait_recv()

    @pl.when(jnp.logical_not(has_prev))
    def _():
        pwkv[...] = jnp.zeros_like(pwkv)

    prev = pwkv[...]
    keys = jnp.concatenate([prev[:, :64], own_pair[:, :64]], axis=0)
    values = jnp.concatenate([prev[:, 64:], own_pair[:, 64:]], axis=0)
    q_row, k_col = iota((T, 2 * T), 0), iota((T, 2 * T), 1)
    usable = (k_col > q_row) & (k_col <= q_row + T) & ((k_col >= T) | has_prev)
    outs = []
    for h in range(2):
        logit = dot_nt(query_w[:, 64 * h : 64 * h + 64], keys) * (0.125 * LOG2E)
        logit = jnp.where(usable, logit, -jnp.inf)
        sink = sinks_s[h] * LOG2E
        top = jnp.maximum(jnp.max(logit, axis=1, keepdims=True), sink)
        weight = jnp.exp2(logit - top)
        norm = jnp.sum(weight, axis=1, keepdims=True) + jnp.exp2(sink - top)
        outs.append(dot((weight / norm).astype(BF16), values))
    win_out = jnp.concatenate(outs, axis=1).astype(BF16).astype(F32)
    with_squares(bb, win_out)
    scaled_w = (win_out * wg_v[...]).astype(BF16)
    for n in range(4):
        bb[:, n * 512 : n * 512 + 512] = dot(scaled_w, wo_w[:, n * 512 : n * 512 + 512]).astype(BF16)

    def scatter(buf, dst, ssem, rsem):
        sends = []
        for d in (4, 5, 3, 2, 6, 7, 1):
            to = (tp + d) % NTP
            rows = buf.at[pl.ds(pl.multiple_of(to * 16, 16), 16), :]
            sends.append(rcopy(rows, dst.at[tp], ssem.at[d], rsem.at[tp], (sp, to)))
        for send in sends:
            send.start()
        return sends

    win_sends = scatter(bb, rb, s_rb, r_rb)

    before, after = (y + NY - 2) % NY, (y + 2) % NY
    row_of = lambda d: (z * NY + (y + d) % NY, tp)
    relays = [
        (before, [(kvb.at[before], 1, r_k.at[before]), (kvb.at[before, 0], 2, r_k4.at[0])]),
        (after, [(kvb.at[after], NY - 1, r_k.at[after]), (kvb.at[after, 1], NY - 2, r_k4.at[1])]),
    ]
    for side, (src, copies) in enumerate(relays):
        rcopy(kvb.at[src], kvb.at[src], s_k.at[0], r_k.at[src], row_of(1)).wait_recv()
        for n, (ref, d, rsem) in enumerate(copies):
            send = rcopy(ref, ref, s_k.at[4 + 2 * side + n], rsem, row_of(d))
            send.start()
            kv_sends.append(send)

    def spread(j):
        key_t, val = kvb[j, 0], kvb[j, 1]
        zero = jnp.zeros_like(key_t)
        feat = iota((T, 128), 0) < 64
        kbd[j, :, :T] = jnp.where(feat, key_t, zero)
        kbd[j, :, T:] = jnp.where(feat, zero, key_t)
        lane = iota((T, 128), 1) < 64
        vbd[j, :T, :] = jnp.where(lane, val, zero)
        vbd[j, T:, :] = jnp.where(lane, zero, val)

    bias_row = jnp.where(iota((1, 2 * T), 1) < T, bias_s[0] * LOG2E, bias_s[1] * LOG2E)

    in_head0 = iota((2 * T, 128), 1) < 64
    far = [(y + d) % NY for d in range(NY)]
    query_pairs = (NZ - z + 1) // 2
    early = jnp.minimum(query_pairs, 2)
    units = 4 * query_pairs

    def unit(i):
        at = jnp.clip(i, 0, units - 1)
        mid, rest = at - 2 * early, jnp.maximum(at - 4 * early, 0)
        p = jnp.where(mid < 0, at // 2, jnp.where(mid < 2 * early, early - 1 - mid // 2, early + rest // 4))
        k = jnp.where(mid < 0, at % 2, jnp.where(mid < 2 * early, 2 + mid % 2, rest % 4))
        real = (i >= 0) & (i < units)
        first = jnp.where(k == 0, y, jnp.where(k == 1, after, jnp.where(k == 2, far[1], far[3])))
        second = jnp.where(k == 0, before, jnp.where(k == 1, far[7], jnp.where(k == 2, far[5], far[4])))
        rows = rows_of(jnp.where(real, z + 2 * p, NZ + 1), 2)
        return p, k, real, (first, second), rows

    halves = (pl.ds(0, 2 * T), pl.ds(2 * T, 2 * T))

    def kv_wait(src):
        rcopy(kvb.at[src], kvb.at[src], s_k.at[0], r_k.at[src], row_of(1)).wait_recv()

    def await_queries(p):
        for n in range(2):
            q = z + 2 * p + n

            @pl.when((q > z) & (q < NZ))
            def _(q=q):
                block = qb.at[rows_of(q), :]
                rcopy(block, block, s_q.at[0], r_q.at[q], (q * NY + y, tp)).wait_recv()

    def total_of(q):
        rows = rows_of(q)
        part, total = parts[NY - 1, rows, :], logs[NY - 1, rows, :]
        for j in range(NY - 2, -1, -1):
            part = part + jnp.exp2(-total) * parts[j, rows, :]
            total = total + logs[j, rows, :]
        flipped = total.T
        return part, (flipped[0:1, :], flipped[64:65, :])

    def p_send(to):
        return rcopy(pout.at[to], prec.at[z], s_p.at[to], r_p.at[z], (to * NY + y, tp))

    def give(zq):
        part, (l0, l1) = total_of(zq)
        pout[zq, :T, :] = part.astype(BF16)
        h0, h1 = l0.astype(BF16).astype(F32), l1.astype(BF16).astype(F32)
        row = iota((16, 128), 0)
        packed = jnp.where(row == 0, h0, jnp.where(row == 1, l0 - h0, jnp.where(row == 2, h1, l1 - h1)))
        pout[zq, T:, :] = packed.astype(BF16)
        p_send(zq).start()

    def unit_step(i, now):
        later = 1 - now
        _, _, _, pair_d, rows_d = unit(i - 4)
        p, _, _, pair, _ = unit(i)
        for half, j in zip(halves, pair_d):
            parts[j, rows_d, :] = dot(weight_b[now, half, :], vbd[j])
        weight_b[later] = jnp.exp2(expo[now]).astype(BF16)
        expo[later] = diff[now] - dot(soft_b[now], tri[...])
        _, _, _, pair_b, rows_b = unit(i - 1)
        for half, j in zip(halves, pair_b):
            score = raw[now, half, :] + bias_row
            soft = jnp.maximum(score, jnp.log(1.0 + jnp.exp2(jnp.minimum(score, 126.0))) * LOG2E)
            diff[later, half, :] = score - soft
            soft_b[later, half, :] = soft.astype(BF16)
            sum0 = jnp.sum(soft[:, :T], axis=1, keepdims=True)
            sum1 = jnp.sum(soft[:, T:], axis=1, keepdims=True)
            logs[j, rows_b, :] = jnp.where(in_head0, sum0, sum1)
        own_rows = rows_of(jnp.minimum(z + 2 * p, NZ - 1), 2)
        for half, j in zip(halves, pair):
            score = dot(qb[own_rows, :], kbd[j])
            limit = jnp.where(p == 0, (y - j) * T, NY * T)
            raw[later, pl.ds(half.start, T), :] = jnp.where(offset[...] < limit, score[:T], -1e30)
            raw[later, pl.ds(half.start + T, T), :] = score[T:]

    def give_done(i):
        p_d, k_d, real_d, _, _ = unit(i)
        for n in range(2):
            q_d = z + 2 * p_d + n

            @pl.when(real_d & (k_d == 3) & (q_d > z) & (q_d < NZ))
            def _(q_d=q_d):
                give(q_d)

    def two_steps(i, _):
        first = 2 * i
        p, k, _, _, _ = unit(first)

        @pl.when((k == 0) & (first < units))
        def _():
            await_queries(p)

        @pl.when(i == 0)
        def _():
            kv_wait(far[7])
            spread(far[7])

        @pl.when(i == early)
        def _():
            for d in (1, 5, 3):
                kv_wait(far[d])
                spread(far[d])
            for n in range(2):
                rcopy(kvb.at[far[4], n], kvb.at[far[4], n], s_k.at[0], r_k4.at[n], row_of(1)).wait_recv()
            spread(far[4])

        unit_step(first, 0)
        unit_step(first + 1, 1)
        give_done(first - 3)
        return 0

    spread(y)
    spread(before)
    spread(after)
    lax.fori_loop(0, 2 * query_pairs + 2, two_steps, 0)

    own_part, own_logs = total_of(z)
    acc_p[...] = own_part

    def merge(i, rows):
        l0, l1 = rows
        src = z - 1 - i
        rcopy(pout.at[src], prec.at[src], s_p.at[0], r_p.at[src], (src * NY + y, tp)).wait_recv()
        factor = jnp.concatenate(
            [jnp.broadcast_to(jnp.exp2(-l0), (64, 128)), jnp.broadcast_to(jnp.exp2(-l1), (64, 128))], axis=0
        ).T
        acc_p[...] += factor * prec[src, :T, :].astype(F32)
        more = prec[src, T:, :].astype(F32)
        return l0 + (more[0:1] + more[1:2]), l1 + (more[2:3] + more[3:4])

    lax.fori_loop(0, z, merge, own_logs)

    stick_out = acc_p[...].astype(BF16).astype(F32)
    with_squares(ab, stick_out)
    scaled_s = (stick_out * sg_v[...]).astype(BF16)
    for n in range(4):
        ab[:, n * 512 : n * 512 + 512] = dot(scaled_s, wo_s[:, n * 512 : n * 512 + 512]).astype(BF16)
    stick_sends = scatter(ab, ra, s_ra, r_ra)

    def gathered(buf, dst, rsem):
        mine = pl.ds(pl.multiple_of(tp * 16, 16), 16)
        total = buf[mine, :].astype(F32)
        for d in (1, 2, 6, 7, 3, 5, 4):
            src = (tp + d) % NTP
            rcopy(dst.at[src], dst.at[src], s_ra.at[0], rsem.at[src], (sp, src)).wait_recv()
            total = total + dst[src].astype(F32)
        scale = lax.rsqrt(jnp.sum(total[:, D:], axis=1, keepdims=True) * (1.0 / 1024) + EPS)
        return total[:, :D] * scale

    combined = gathered(bb, rb, r_rb)
    combined = combined + gathered(ab, ra, r_ra)
    mean = jnp.sum(combined * combined, axis=1, keepdims=True) * (1.0 / D)
    out[...] = (combined * lax.rsqrt(mean + EPS) * post_v[...]).astype(BF16)

    for send in tok_sends + kv_sends + win_sends + stick_sends:
        send.wait_send()

    @pl.when(has_next)
    def _():
        win_send.wait_send()

    for n in (4, 5, 6):
        rcopy(own_tok, own_tok, s_a.at[n], r_a.at[tp], (sp, partner)).wait_send()

    def q_drain(i, _):
        q_send(i).wait_send()
        return 0

    lax.fori_loop(0, z, q_drain, 0)

    def p_drain(i, _):
        p_send(NZ - 1 - i).wait_send()
        return 0

    lax.fori_loop(0, NZ - 1 - z, p_drain, 0)


def shards(
    tokens, pre_gain, w_query_stick, w_key_stick, w_value_stick, w_query_window, w_key_window, w_value_window,
    stick_bias, sinks, stick_gain, window_gain, w_out_stick, w_out_window, post_gain,
):
    anywhere = pl.BlockSpec(memory_space=pl.ANY)
    dma = pltpu.SemaphoreType.DMA
    vm = pltpu.VMEM
    scratch = [
        vm((NTP, T, CH), BF16), vm((D, 512), BF16), vm((128, D), BF16),
        vm((128, D), BF16), vm((128, D), BF16), vm((1, D), F32), vm((1, 128), F32), vm((1, 128), F32), vm((1, D), F32),
        vm((T, 512), F32), vm((T, 128), F32), vm((T, 128), F32),
        vm((NY, 2, T, 128), BF16), vm(((NZ + 1) * T, 128), BF16), vm((NY, 128, 2 * T), BF16), vm((NY, 2 * T, 128), BF16),
        vm((256, 256), BF16), vm((2, 4 * T, 2 * T), F32), vm((2, 4 * T, 2 * T), BF16), vm((2, 4 * T, 2 * T), F32),
        vm((2, 4 * T, 2 * T), F32), vm((2, 4 * T, 2 * T), BF16),
        vm((NY, (NZ + 3) * T, 128), F32), vm((NY, (NZ + 3) * T, 128), F32), vm((T, 2 * T), jnp.int32),
        vm((T, 128), BF16), vm((T, 128), BF16), vm((NZ, PROWS, 128), BF16), vm((NZ, PROWS, 128), BF16),
        vm((T, 128), F32), vm((T, PACK), BF16), vm((T, PACK), BF16),
        vm((NTP, 16, PACK), BF16), vm((NTP, 16, PACK), BF16), pltpu.SMEM((2,), F32), pltpu.SMEM((2,), F32),
        dma((15,)), dma((7,)), dma((NTP,)), dma((8,)), dma((NY,)), dma((2,)), dma((NZ,)), dma((NZ,)), dma, dma, pltpu.SemaphoreType.REGULAR,
        dma((NZ,)), dma((NZ,)), dma((NTP,)), dma((NTP,)), dma((NTP,)), dma((NTP,)),
    ]
    return pl.pallas_call(
        kernel,
        out_shape=jax.ShapeDtypeStruct((T // NTP, D), BF16),
        in_specs=[anywhere] * 15,
        out_specs=pl.BlockSpec(memory_space=pltpu.VMEM),
        scratch_shapes=scratch,
        compiler_params=pltpu.CompilerParams(
            collective_id=0, has_side_effects=True, vmem_limit_bytes=60 * 1024 * 1024
        ),
    )(
        tokens, pre_gain.reshape(1, -1), w_query_stick, w_key_stick, w_value_stick, w_query_window,
        w_key_window.T, w_value_window.T, stick_bias, sinks, stick_gain.reshape(1, -1), window_gain.reshape(1, -1),
        w_out_stick, w_out_window, post_gain.reshape(1, -1),
    )


def solution(mesh):
    in_specs = (
        P("sp", "tp"),
        P(),
        P(None, "tp"),
        P(None, "tp"),
        P(None, "tp"),
        P(None, "tp"),
        P(None, "tp"),
        P(None, "tp"),
        P("tp"),
        P("tp"),
        P("tp"),
        P("tp"),
        P("tp", None),
        P("tp", None),
        P(),
    )
    out_specs = P(("sp", "tp"), None)
    return jax.shard_map(shards, mesh=mesh, in_specs=in_specs, out_specs=out_specs, check_vma=False)
```

```python
import functools

import jax
import jax.numpy as jnp
from jax import lax
from jax.experimental import pallas as pl
from jax.experimental.pallas import tpu as pltpu
from jax.sharding import PartitionSpec as P

T = 128
D = 2048
CH = 256
NY = 8
NZ = 8
NTP = 8
NX = 4
LOG2E = 1.4426950408889634
EPS = 1e-06
PACK = D + 128
PROWS = T + 16
MESH = pl.DeviceIdType.MESH
F32 = jnp.float32
BF16 = jnp.bfloat16


def dot(a, b):
    return jnp.dot(a, b, preferred_element_type=F32)


def dot_nt(a, b):
    return lax.dot_general(a, b, (((1,), (1,)), ((), ())), preferred_element_type=F32)


def iota(shape, dim):
    return lax.broadcasted_iota(jnp.int32, shape, dim)


def split(total):
    high = total.astype(BF16).astype(F32)
    lane = iota((total.shape[0], 128), 1)
    return jnp.where(lane == 0, high, jnp.where(lane == 1, total - high, 0.0)).astype(BF16)


def kernel(
    tok, pre, wqs, wks, wvs, wqw, wkw, wvw, bias, sinks, sgain, wgain, wos, wow, post,
    out,
    tok_all, w4, w_win, wo_s, wo_w, pre_v, sg_v, wg_v, post_v,
    acc4, acc_w, sq, kvb, qb, kbd, vbd, tri, raw, soft_b, diff, expo, weight_b, parts, logs, offset,
    wkv, pwkv, pout, prec, acc_p, ab, bb, ra, rb, mix_a, mix_b, in_a, in_b, bias_s, sinks_s,
    lsem, s_a, r_a, s_k, r_k, r_k2, r_k3, r_k4, s_q, r_q, s_w, r_w, ready, s_p, r_p, s_ra, r_ra, s_rb, r_rb,
    s_pair, r_pair,
):
    sp = lax.axis_index("sp")
    tp = lax.axis_index("tp")
    z = sp // NY
    y = sp % NY
    x = tp // 2
    c = tp % 2

    def rcopy(src, dst, ssem, rsem, dev):
        return pltpu.make_async_remote_copy(
            src_ref=src, dst_ref=dst, send_sem=ssem, recv_sem=rsem, device_id=dev, device_id_type=MESH
        )

    def rows_of(block, count=1):
        return pl.ds(pl.multiple_of(block * T, T), count * T)

    loads = [pltpu.make_async_copy(tok, tok_all.at[tp], lsem.at[0])]
    pairs = [
        (pre, pre_v), (wks, w4.at[:, pl.ds(0, 128)]), (wvs, w4.at[:, pl.ds(128, 128)]),
        (wqs, w4.at[:, pl.ds(256, 128)]), (wqw, w4.at[:, pl.ds(384, 128)]),
        (wkw, w_win.at[pl.ds(0, 64), :]), (wvw, w_win.at[pl.ds(64, 64), :]),
        (bias, bias_s), (sinks, sinks_s), (sgain, sg_v), (wgain, wg_v), (post, post_v), (wos, wo_s.at[c]), (wow, wo_w.at[c]),
    ]
    for n, (src, dst) in enumerate(pairs):
        loads.append(pltpu.make_async_copy(src, dst, lsem.at[n + 1]))
    for load in loads:
        load.start()

    barrier = pltpu.get_barrier_semaphore()

    def greet(dev):
        pl.semaphore_signal(barrier, inc=1, device_id=dev, device_id_type=MESH)

    greeted = [(sp, (tp + d) % NTP) for d in range(1, NTP)]
    greeted += [(z * NY + (y + d) % NY, tp) for d in (1, 2, NY - 2, NY - 1)]
    for dev in greeted:
        greet(dev)

    def greet_row(i, _):
        greet((i * NY + y, tp))
        return 0

    lax.fori_loop(z + 1, NZ, greet_row, 0)
    has_next = sp < NY * NZ - 1
    has_prev = sp > 0
    starts_row = (y == 0) & has_prev
    ends_row = (y == NY - 1) & has_next
    nxt = ((sp + 1) % (NY * NZ), tp)
    before_me = ((sp + NY * NZ - 1) % (NY * NZ), tp)

    @pl.when(ends_row)
    def _():
        greet(nxt)

    row2, col2 = iota((256, 256), 0), iota((256, 256), 1)
    tri[...] = jnp.where((row2 > col2) & (row2 // T == col2 // T), 1.0, 0.0).astype(BF16)
    offset[...] = iota((T, 2 * T), 1) % T - iota((T, 2 * T), 0)
    acc4[...] = jnp.zeros_like(acc4)
    acc_w[...] = jnp.zeros_like(acc_w)
    sq[...] = jnp.zeros_like(sq)
    for ref in (raw, soft_b, diff, expo, weight_b):
        ref[...] = jnp.zeros_like(ref)
    qb[NZ * T :, :] = jnp.zeros((T, 128), BF16)

    pl.semaphore_wait(barrier, len(greeted) + z + jnp.where(starts_row, 1, 0))

    @pl.when(starts_row)
    def _():
        pl.semaphore_signal(ready, inc=1, device_id=before_me, device_id_type=MESH)

    loads[0].wait()

    partner = x * 2 + (1 - c)
    own_tok = tok_all.at[tp]
    tok_sends = []
    for n, d in enumerate((2, 1, 3)):
        peer = ((x + d) % NX) * 2 + c
        tok_sends.append(rcopy(own_tok, own_tok, s_a.at[n], r_a.at[tp], (sp, peer)))
    tok_sends.append(rcopy(own_tok, own_tok, s_a.at[3], r_a.at[tp], (sp, partner)))
    for send in tok_sends:
        send.start()
    for load in loads[1:8]:
        load.wait()

    def feature_step(i, _):
        dist = jnp.where(i < 2, 0, jnp.where((i == 2) | (i == 5), 1, jnp.where((i == 3) | (i == 6), 3, 2)))
        core = jnp.where((i == 1) | (i >= 5), 1 - c, c)
        src = ((x + dist) % NX) * 2 + core
        block = tok_all.at[src]

        @pl.when(i > 0)
        def _():
            rcopy(block, block, s_a.at[0], r_a.at[src], (sp, partner)).wait_recv()

        @pl.when((i >= 2) & (i <= 4))
        def _():
            rcopy(block, block, s_a.at[i + 2], r_a.at[src], (sp, partner)).start()

        feats = block[...].astype(F32)
        sq[...] += feats[:, :128] * feats[:, :128] + feats[:, 128:] * feats[:, 128:]
        at = pl.ds(pl.multiple_of(src * CH, CH), CH)
        scaled = (feats * pre_v[:, at]).astype(BF16)
        acc4[...] += dot(scaled, w4[at, :])
        acc_w[...] += dot_nt(scaled, w_win[:, at])
        return 0

    lax.fori_loop(0, NTP, feature_step, 0)
    inv = lax.rsqrt(jnp.sum(sq[...], axis=1, keepdims=True) * (1.0 / D) + EPS)

    own_pair = (acc_w[...] * inv).astype(BF16)
    wkv[...] = own_pair

    @pl.when(ends_row)
    def _():
        pl.semaphore_wait(ready, 1)

    win_send = rcopy(wkv, pwkv, s_w, r_w, nxt)

    @pl.when(has_next)
    def _():
        win_send.start()

    kvb[y, 0] = (acc4[:, 0:128] * inv).T.astype(BF16)
    kvb[y, 1] = (acc4[:, 128:256] * inv).astype(BF16)
    own_kv = kvb.at[y]
    row_of = lambda d: (z * NY + (y + d) % NY, tp)
    kv_sends = []
    for plane in range(2):
        for side, d in enumerate((2, NY - 2)):
            ref = kvb.at[y, plane]
            kv_sends.append(rcopy(ref, ref, s_k.at[2 * plane + side], r_k2.at[side, plane], row_of(d)))
    for n, d in enumerate((1, NY - 1)):
        kv_sends.append(rcopy(own_kv, own_kv, s_k.at[4 + n], r_k.at[y], row_of(d)))
    for send in kv_sends:
        send.start()
    qb[rows_of(z), :] = (acc4[:, 256:384] * (inv * (0.125 * LOG2E))).astype(BF16)

    def q_send(i):
        return rcopy(qb.at[rows_of(z), :], qb.at[rows_of(z), :], s_q.at[i], r_q.at[z], (i * NY + y, tp))

    def q_start(i, _):
        q_send(i).start()
        return 0

    lax.fori_loop(0, z, q_start, 0)

    for load in loads[8:]:
        load.wait()
    pair_sends = []
    for n, ref in enumerate((wo_w.at[c], wo_s.at[c])):
        pair_sends.append(rcopy(ref, ref, s_pair.at[n], r_pair.at[n], (sp, partner)))
    for send in pair_sends:
        send.start()

    query_w = (acc4[:, 384:512] * inv).astype(BF16)

    @pl.when(has_prev)
    def _():
        rcopy(wkv, pwkv, s_w, r_w, before_me).wait_recv()

    @pl.when(jnp.logical_not(has_prev))
    def _():
        pwkv[...] = jnp.zeros_like(pwkv)

    prev = pwkv[...]
    keys = jnp.concatenate([prev[:, :64], own_pair[:, :64]], axis=0)
    values = jnp.concatenate([prev[:, 64:], own_pair[:, 64:]], axis=0)
    q_row, k_col = iota((T, 2 * T), 0), iota((T, 2 * T), 1)
    usable = (k_col > q_row) & (k_col <= q_row + T) & ((k_col >= T) | has_prev)
    outs = []
    for h in range(2):
        logit = dot_nt(query_w[:, 64 * h : 64 * h + 64], keys) * (0.125 * LOG2E)
        logit = jnp.where(usable, logit, -jnp.inf)
        sink = sinks_s[h] * LOG2E
        top = jnp.maximum(jnp.max(logit, axis=1, keepdims=True), sink)
        weight = jnp.exp2(logit - top)
        norm = jnp.sum(weight, axis=1, keepdims=True) + jnp.exp2(sink - top)
        outs.append(dot((weight / norm).astype(BF16), values))
    win_out = jnp.concatenate(outs, axis=1).astype(BF16).astype(F32)

    def project_out(result, gain, weight, mix, inbound, buf, dst, slot, ssem, rsem):
        scaled = (result * gain[...]).astype(BF16)
        sums = split(jnp.sum(result * result, axis=1, keepdims=True))
        for core in range(2):
            for chip in range(NX):
                rows = slice(32 * chip + 16 * core, 32 * chip + 16 * core + 16)
                mix[core, 16 * chip : 16 * chip + 16, :128] = scaled[rows]
                mix[core, 16 * chip : 16 * chip + 16, 128:] = sums[rows]
        over = rcopy(mix.at[1 - c], inbound, s_pair.at[2 + slot], r_pair.at[2 + slot], (sp, partner))
        over.start()
        theirs_w = weight.at[1 - c]
        rcopy(theirs_w, theirs_w, s_pair.at[0], r_pair.at[slot], (sp, partner)).wait_recv()
        mine = mix[c, :, :128]
        own = [dot(mine, weight[c, :, n * 512 : n * 512 + 512]) for n in range(4)]
        over.wait_recv()
        theirs = inbound[:, :128]
        for n in range(4):
            part = own[n] + dot(theirs, weight[1 - c, :, n * 512 : n * 512 + 512])
            buf[:, n * 512 : n * 512 + 512] = part.astype(BF16)
        both = mix[c, :, 128:].astype(F32) + inbound[:, 128:].astype(F32)
        buf[:, D:] = split(jnp.sum(both, axis=1, keepdims=True))
        sends = []
        for d in (2, 1, 3):
            to = (x + d) % NX
            rows = buf.at[pl.ds(pl.multiple_of(to * 16, 16), 16), :]
            sends.append(rcopy(rows, dst.at[x], ssem.at[d], rsem.at[x], (sp, to * 2 + c)))
        for send in sends:
            send.start()
        return sends + [over]

    win_sends = project_out(win_out, wg_v, wo_w, mix_b, in_b, bb, rb, 0, s_rb, r_rb)

    before, after = (y + NY - 2) % NY, (y + 2) % NY
    for plane in range(2):
        for side, src in enumerate((before, after)):
            ref = kvb.at[src, plane]
            rcopy(ref, ref, s_k.at[0], r_k2.at[side, plane], row_of(1)).wait_recv()
            if side == plane:
                send = rcopy(ref, ref, s_k.at[6 + side], r_k4.at[side], row_of((2, NY - 2)[side]))
                send.start()
                kv_sends.append(send)
            send = rcopy(ref, ref, s_k.at[8 + 2 * side + plane], r_k3.at[side, plane], row_of((1, NY - 1)[side]))
            send.start()
            kv_sends.append(send)

    def spread(j):
        key_t, val = kvb[j, 0], kvb[j, 1]
        zero = jnp.zeros_like(key_t)
        feat = iota((T, 128), 0) < 64
        kbd[j, :, :T] = jnp.where(feat, key_t, zero)
        kbd[j, :, T:] = jnp.where(feat, zero, key_t)
        lane = iota((T, 128), 1) < 64
        vbd[j, :T, :] = jnp.where(lane, val, zero)
        vbd[j, T:, :] = jnp.where(lane, zero, val)

    bias_row = jnp.where(iota((1, 2 * T), 1) < T, bias_s[0] * LOG2E, bias_s[1] * LOG2E)

    in_head0 = iota((2 * T, 128), 1) < 64
    far = [(y + d) % NY for d in range(NY)]
    query_pairs = (NZ - z + 1) // 2
    early = jnp.minimum(query_pairs, 2)
    units = 4 * query_pairs

    def unit(i):
        at = jnp.clip(i, 0, units - 1)
        mid, rest = at - 2 * early, jnp.maximum(at - 4 * early, 0)
        p = jnp.where(mid < 0, at // 2, jnp.where(mid < 2 * early, early - 1 - mid // 2, early + rest // 4))
        k = jnp.where(mid < 0, at % 2, jnp.where(mid < 2 * early, 2 + mid % 2, rest % 4))
        real = (i >= 0) & (i < units)
        first = jnp.where(k == 0, y, jnp.where(k == 1, after, jnp.where(k == 2, far[1], far[3])))
        second = jnp.where(k == 0, before, jnp.where(k == 1, far[7], jnp.where(k == 2, far[5], far[4])))
        rows = rows_of(jnp.where(real, z + 2 * p, NZ + 1), 2)
        return p, k, real, (first, second), rows

    halves = (pl.ds(0, 2 * T), pl.ds(2 * T, 2 * T))

    def kv_wait(src):
        rcopy(kvb.at[src], kvb.at[src], s_k.at[0], r_k.at[src], row_of(1)).wait_recv()

    def await_queries(p):
        for n in range(2):
            q = z + 2 * p + n

            @pl.when((q > z) & (q < NZ))
            def _(q=q):
                block = qb.at[rows_of(q), :]
                rcopy(block, block, s_q.at[0], r_q.at[q], (q * NY + y, tp)).wait_recv()

    def total_of(q):
        rows = rows_of(q)
        part, total = parts[NY - 1, rows, :], logs[NY - 1, rows, :]
        for j in range(NY - 2, -1, -1):
            part = part + jnp.exp2(-total) * parts[j, rows, :]
            total = total + logs[j, rows, :]
        flipped = total.T
        return part, (flipped[0:1, :], flipped[64:65, :])

    def p_send(to):
        return rcopy(pout.at[to], prec.at[z], s_p.at[to], r_p.at[z], (to * NY + y, tp))

    def give(zq):
        part, (l0, l1) = total_of(zq)
        pout[zq, :T, :] = part.astype(BF16)
        h0, h1 = l0.astype(BF16).astype(F32), l1.astype(BF16).astype(F32)
        row = iota((16, 128), 0)
        packed = jnp.where(row == 0, h0, jnp.where(row == 1, l0 - h0, jnp.where(row == 2, h1, l1 - h1)))
        pout[zq, T:, :] = packed.astype(BF16)
        p_send(zq).start()

    def unit_step(i, now):
        later = 1 - now
        _, _, _, pair_d, rows_d = unit(i - 4)
        p, _, _, pair, _ = unit(i)
        for half, j in zip(halves, pair_d):
            parts[j, rows_d, :] = dot(weight_b[now, half, :], vbd[j])
        weight_b[later] = jnp.exp2(expo[now]).astype(BF16)
        expo[later] = diff[now] - dot(soft_b[now], tri[...])
        _, _, _, pair_b, rows_b = unit(i - 1)
        for half, j in zip(halves, pair_b):
            score = raw[now, half, :] + bias_row
            soft = jnp.maximum(score, jnp.log(1.0 + jnp.exp2(jnp.minimum(score, 126.0))) * LOG2E)
            diff[later, half, :] = score - soft
            soft_b[later, half, :] = soft.astype(BF16)
            sum0 = jnp.sum(soft[:, :T], axis=1, keepdims=True)
            sum1 = jnp.sum(soft[:, T:], axis=1, keepdims=True)
            logs[j, rows_b, :] = jnp.where(in_head0, sum0, sum1)
        own_rows = rows_of(jnp.minimum(z + 2 * p, NZ - 1), 2)
        for half, j in zip(halves, pair):
            score = dot(qb[own_rows, :], kbd[j])
            limit = jnp.where(p == 0, (y - j) * T, NY * T)
            raw[later, pl.ds(half.start, T), :] = jnp.where(offset[...] < limit, score[:T], -1e30)
            raw[later, pl.ds(half.start + T, T), :] = score[T:]

    def give_done(i):
        p_d, k_d, real_d, _, _ = unit(i)
        for n in range(2):
            q_d = z + 2 * p_d + n

            @pl.when(real_d & (k_d == 3) & (q_d > z) & (q_d < NZ))
            def _(q_d=q_d):
                give(q_d)

    def two_steps(i, _):
        first = 2 * i
        p, k, _, _, _ = unit(first)

        @pl.when((k == 0) & (first < units))
        def _():
            await_queries(p)

        @pl.when(i == 0)
        def _():
            kv_wait(far[7])
            spread(far[7])

        @pl.when(i == early)
        def _():
            kv_wait(far[1])
            spread(far[1])
            for side, src in enumerate((far[5], far[3])):
                for plane in range(2):
                    ref = kvb.at[src, plane]
                    rcopy(ref, ref, s_k.at[0], r_k3.at[side, plane], row_of(1)).wait_recv()
                spread(src)
            for n in range(2):
                rcopy(kvb.at[far[4], n], kvb.at[far[4], n], s_k.at[0], r_k4.at[n], row_of(1)).wait_recv()
            spread(far[4])

        unit_step(first, 0)
        unit_step(first + 1, 1)
        give_done(first - 3)
        return 0

    spread(y)
    spread(before)
    spread(after)
    lax.fori_loop(0, 2 * query_pairs + 2, two_steps, 0)

    own_part, own_logs = total_of(z)
    acc_p[...] = own_part

    def merge(i, rows):
        l0, l1 = rows
        src = z - 1 - i
        rcopy(pout.at[src], prec.at[src], s_p.at[0], r_p.at[src], (src * NY + y, tp)).wait_recv()
        factor = jnp.concatenate(
            [jnp.broadcast_to(jnp.exp2(-l0), (64, 128)), jnp.broadcast_to(jnp.exp2(-l1), (64, 128))], axis=0
        ).T
        acc_p[...] += factor * prec[src, :T, :].astype(F32)
        more = prec[src, T:, :].astype(F32)
        return l0 + (more[0:1] + more[1:2]), l1 + (more[2:3] + more[3:4])

    lax.fori_loop(0, z, merge, own_logs)

    stick_out = acc_p[...].astype(BF16).astype(F32)
    stick_sends = project_out(stick_out, sg_v, wo_s, mix_a, in_a, ab, ra, 1, s_ra, r_ra)

    def gathered(buf, dst, rsem):
        total = buf[pl.ds(pl.multiple_of(x * 16, 16), 16), :].astype(F32)
        for d in (1, 3, 2):
            src = (x + d) % NX
            rcopy(dst.at[src], dst.at[src], s_ra.at[0], rsem.at[src], (sp, src * 2 + c)).wait_recv()
            total = total + dst[src].astype(F32)
        scale = lax.rsqrt(jnp.sum(total[:, D:], axis=1, keepdims=True) * (1.0 / 1024) + EPS)
        return total[:, :D] * scale

    combined = gathered(bb, rb, r_rb)
    combined = combined + gathered(ab, ra, r_ra)
    mean = jnp.sum(combined * combined, axis=1, keepdims=True) * (1.0 / D)
    out[...] = (combined * lax.rsqrt(mean + EPS) * post_v[...]).astype(BF16)

    for send in tok_sends + kv_sends + pair_sends + win_sends + stick_sends:
        send.wait_send()

    @pl.when(has_next)
    def _():
        win_send.wait_send()

    for n in (4, 5, 6):
        rcopy(own_tok, own_tok, s_a.at[n], r_a.at[tp], (sp, partner)).wait_send()

    def q_drain(i, _):
        q_send(i).wait_send()
        return 0

    lax.fori_loop(0, z, q_drain, 0)

    def p_drain(i, _):
        p_send(NZ - 1 - i).wait_send()
        return 0

    lax.fori_loop(0, NZ - 1 - z, p_drain, 0)


def shards(
    tokens, pre_gain, w_query_stick, w_key_stick, w_value_stick, w_query_window, w_key_window, w_value_window,
    stick_bias, sinks, stick_gain, window_gain, w_out_stick, w_out_window, post_gain,
):
    anywhere = pl.BlockSpec(memory_space=pl.ANY)
    dma = pltpu.SemaphoreType.DMA
    vm = pltpu.VMEM
    scratch = [
        vm((NTP, T, CH), BF16), vm((D, 512), BF16), vm((128, D), BF16),
        vm((2, 128, D), BF16), vm((2, 128, D), BF16), vm((1, D), F32), vm((1, 128), F32), vm((1, 128), F32), vm((1, D), F32),
        vm((T, 512), F32), vm((T, 128), F32), vm((T, 128), F32),
        vm((NY, 2, T, 128), BF16), vm(((NZ + 1) * T, 128), BF16), vm((NY, 128, 2 * T), BF16), vm((NY, 2 * T, 128), BF16),
        vm((256, 256), BF16), vm((2, 4 * T, 2 * T), F32), vm((2, 4 * T, 2 * T), BF16), vm((2, 4 * T, 2 * T), F32),
        vm((2, 4 * T, 2 * T), F32), vm((2, 4 * T, 2 * T), BF16),
        vm((NY, (NZ + 3) * T, 128), F32), vm((NY, (NZ + 3) * T, 128), F32), vm((T, 2 * T), jnp.int32),
        vm((T, 128), BF16), vm((T, 128), BF16), vm((NZ, PROWS, 128), BF16), vm((NZ, PROWS, 128), BF16),
        vm((T, 128), F32), vm((64, PACK), BF16), vm((64, PACK), BF16),
        vm((NX, 16, PACK), BF16), vm((NX, 16, PACK), BF16), vm((2, 64, 256), BF16), vm((2, 64, 256), BF16),
        vm((64, 256), BF16), vm((64, 256), BF16), pltpu.SMEM((2,), F32), pltpu.SMEM((2,), F32),
        dma((15,)), dma((7,)), dma((NTP,)), dma((12,)), dma((NY,)), dma((2, 2)), dma((2, 2)), dma((2,)), dma((NZ,)), dma((NZ,)), dma, dma, pltpu.SemaphoreType.REGULAR,
        dma((NZ,)), dma((NZ,)), dma((NX,)), dma((NX,)), dma((NX,)), dma((NX,)), dma((4,)), dma((4,)),
    ]
    return pl.pallas_call(
        kernel,
        out_shape=jax.ShapeDtypeStruct((T // NTP, D), BF16),
        in_specs=[anywhere] * 15,
        out_specs=pl.BlockSpec(memory_space=pltpu.VMEM),
        scratch_shapes=scratch,
        compiler_params=pltpu.CompilerParams(
            collective_id=0, has_side_effects=True, vmem_limit_bytes=60 * 1024 * 1024
        ),
    )(
        tokens, pre_gain.reshape(1, -1), w_query_stick, w_key_stick, w_value_stick, w_query_window,
        w_key_window.T, w_value_window.T, stick_bias, sinks, stick_gain.reshape(1, -1), window_gain.reshape(1, -1),
        w_out_stick, w_out_window, post_gain.reshape(1, -1),
    )


def solution(mesh):
    in_specs = (
        P("sp", "tp"),
        P(),
        P(None, "tp"),
        P(None, "tp"),
        P(None, "tp"),
        P(None, "tp"),
        P(None, "tp"),
        P(None, "tp"),
        P("tp"),
        P("tp"),
        P("tp"),
        P("tp"),
        P("tp", None),
        P("tp", None),
        P(),
    )
    out_specs = P(("sp", "tp"), None)
    return jax.shard_map(shards, mesh=mesh, in_specs=in_specs, out_specs=out_specs, check_vma=False)
```

```python
import functools

import jax
import jax.numpy as jnp
from jax import lax
from jax.experimental import pallas as pl
from jax.experimental.pallas import tpu as pltpu
from jax.sharding import PartitionSpec as P

T = 128
D = 2048
CH = 256
NY = 8
NZ = 8
NTP = 8
NX = 4
LOG2E = 1.4426950408889634
EPS = 1e-06
PACK = D + 128
MESH = pl.DeviceIdType.MESH
F32 = jnp.float32
BF16 = jnp.bfloat16


def dot(a, b):
    return jnp.dot(a, b, preferred_element_type=F32)


def dot_nt(a, b):
    return lax.dot_general(a, b, (((1,), (1,)), ((), ())), preferred_element_type=F32)


def iota(shape, dim):
    return lax.broadcasted_iota(jnp.int32, shape, dim)


def split(total):
    high = total.astype(BF16).astype(F32)
    lane = iota((total.shape[0], 128), 1)
    return jnp.where(lane == 0, high, jnp.where(lane == 1, total - high, 0.0)).astype(BF16)


def kernel(
    tok, pre, wqs, wks, wvs, wqw, wkw, wvw, bias, sinks, sgain, wgain, wos, wow, post,
    out,
    tok_all, w4, w_win, wo_s, wo_w, pre_v, sg_v, wg_v, post_v,
    acc4, acc_w, sq, kvb, qb, kbd, vbd, tri, raw, soft_b, diff, expo, weight_b, parts, logs, offset,
    wkv, pwkv, pout, prec, lout, lrec, acc_p, ab, bb, ra, rb, mix_a, mix_b, in_a, in_b, bias_s, sinks_s,
    lsem, s_a, r_a, s_k, r_k, r_k2, r_k3, r_k4, s_q, r_q, s_w, r_w, ready, s_p, r_p, s_l, r_l, s_ra, r_ra, s_rb, r_rb,
    s_pair, r_pair,
):
    sp = lax.axis_index("sp")
    tp = lax.axis_index("tp")
    z = sp // NY
    y = sp % NY
    x = tp // 2
    c = tp % 2

    def rcopy(src, dst, ssem, rsem, dev):
        return pltpu.make_async_remote_copy(
            src_ref=src, dst_ref=dst, send_sem=ssem, recv_sem=rsem, device_id=dev, device_id_type=MESH
        )

    def rows_of(block, count=1):
        return pl.ds(pl.multiple_of(block * T, T), count * T)

    loads = [pltpu.make_async_copy(tok, tok_all.at[tp], lsem.at[0])]
    pairs = [
        (pre, pre_v), (wks, w4.at[:, pl.ds(0, 128)]), (wvs, w4.at[:, pl.ds(128, 128)]),
        (wqs, w4.at[:, pl.ds(256, 128)]), (wqw, w4.at[:, pl.ds(384, 128)]),
        (wkw, w_win.at[pl.ds(0, 64), :]), (wvw, w_win.at[pl.ds(64, 64), :]),
        (bias, bias_s), (sinks, sinks_s), (sgain, sg_v), (wgain, wg_v), (post, post_v), (wos, wo_s.at[c]), (wow, wo_w.at[c]),
    ]
    for n, (src, dst) in enumerate(pairs):
        loads.append(pltpu.make_async_copy(src, dst, lsem.at[n + 1]))
    for load in loads:
        load.start()

    barrier = pltpu.get_barrier_semaphore()

    def greet(dev):
        pl.semaphore_signal(barrier, inc=1, device_id=dev, device_id_type=MESH)

    greeted = [(sp, (tp + d) % NTP) for d in range(1, NTP)]
    greeted += [(z * NY + (y + d) % NY, tp) for d in (1, 2, NY - 2, NY - 1)]
    for dev in greeted:
        greet(dev)

    def greet_row(i, _):
        greet((i * NY + y, tp))
        return 0

    lax.fori_loop(z + 1, NZ, greet_row, 0)
    has_next = sp < NY * NZ - 1
    has_prev = sp > 0
    starts_row = (y == 0) & has_prev
    ends_row = (y == NY - 1) & has_next
    nxt = ((sp + 1) % (NY * NZ), tp)
    before_me = ((sp + NY * NZ - 1) % (NY * NZ), tp)

    @pl.when(ends_row)
    def _():
        greet(nxt)

    row2, col2 = iota((256, 256), 0), iota((256, 256), 1)
    tri[...] = jnp.where((row2 > col2) & (row2 // T == col2 // T), 1.0, 0.0).astype(BF16)
    offset[...] = iota((T, 2 * T), 1) % T - iota((T, 2 * T), 0)
    acc4[...] = jnp.zeros_like(acc4)
    acc_w[...] = jnp.zeros_like(acc_w)
    sq[...] = jnp.zeros_like(sq)
    for ref in (raw, soft_b, diff, expo, weight_b):
        ref[...] = jnp.zeros_like(ref)
    qb[NZ * T :, :] = jnp.zeros((T, 128), BF16)

    pl.semaphore_wait(barrier, len(greeted) + z + jnp.where(starts_row, 1, 0))

    @pl.when(starts_row)
    def _():
        pl.semaphore_signal(ready, inc=1, device_id=before_me, device_id_type=MESH)

    loads[0].wait()

    partner = x * 2 + (1 - c)
    own_tok = tok_all.at[tp]
    tok_sends = []
    for n, d in enumerate((2, 1, 3)):
        peer = ((x + d) % NX) * 2 + c
        tok_sends.append(rcopy(own_tok, own_tok, s_a.at[n], r_a.at[tp], (sp, peer)))
    tok_sends.append(rcopy(own_tok, own_tok, s_a.at[3], r_a.at[tp], (sp, partner)))
    for send in tok_sends:
        send.start()
    for load in loads[1:8]:
        load.wait()

    def feature_step(i, _):
        dist = jnp.where(i < 2, 0, jnp.where((i == 2) | (i == 5), 1, jnp.where((i == 3) | (i == 6), 3, 2)))
        core = jnp.where((i == 1) | (i >= 5), 1 - c, c)
        src = ((x + dist) % NX) * 2 + core
        block = tok_all.at[src]

        @pl.when(i > 0)
        def _():
            rcopy(block, block, s_a.at[0], r_a.at[src], (sp, partner)).wait_recv()

        @pl.when((i >= 2) & (i <= 4))
        def _():
            rcopy(block, block, s_a.at[i + 2], r_a.at[src], (sp, partner)).start()

        feats = block[...].astype(F32)
        sq[...] += feats[:, :128] * feats[:, :128] + feats[:, 128:] * feats[:, 128:]
        at = pl.ds(pl.multiple_of(src * CH, CH), CH)
        scaled = (feats * pre_v[:, at]).astype(BF16)
        acc4[...] += dot(scaled, w4[at, :])
        acc_w[...] += dot_nt(scaled, w_win[:, at])
        return 0

    lax.fori_loop(0, NTP, feature_step, 0)
    inv = lax.rsqrt(jnp.sum(sq[...], axis=1, keepdims=True) * (1.0 / D) + EPS)

    kvb[y, 0] = (acc4[:, 0:128] * inv).T.astype(BF16)
    kvb[y, 1] = (acc4[:, 128:256] * inv).astype(BF16)
    own_kv = kvb.at[y]
    row_of = lambda d: (z * NY + (y + d) % NY, tp)
    kv_sends = []
    for plane in range(2):
        for side, d in enumerate((2, NY - 2)):
            ref = kvb.at[y, plane]
            kv_sends.append(rcopy(ref, ref, s_k.at[2 * plane + side], r_k2.at[side, plane], row_of(d)))
    for send in kv_sends:
        send.start()
    own_pair = (acc_w[...] * inv).astype(BF16)
    wkv[...] = own_pair

    @pl.when(ends_row)
    def _():
        pl.semaphore_wait(ready, 1)

    win_send = rcopy(wkv, pwkv, s_w, r_w, nxt)

    @pl.when(has_next)
    def _():
        win_send.start()

    for n, d in enumerate((1, NY - 1)):
        send = rcopy(own_kv, own_kv, s_k.at[4 + n], r_k.at[y], row_of(d))
        send.start()
        kv_sends.append(send)
    qb[rows_of(z), :] = (acc4[:, 256:384] * (inv * (0.125 * LOG2E))).astype(BF16)

    def q_send(i):
        return rcopy(qb.at[rows_of(z), :], qb.at[rows_of(z), :], s_q.at[i], r_q.at[z], (i * NY + y, tp))

    def q_start(i, _):
        q_send(i).start()
        return 0

    lax.fori_loop(0, z, q_start, 0)

    for load in loads[8:]:
        load.wait()
    pair_sends = []
    for n, ref in enumerate((wo_w.at[c], wo_s.at[c])):
        pair_sends.append(rcopy(ref, ref, s_pair.at[n], r_pair.at[n], (sp, partner)))
    for send in pair_sends:
        send.start()

    before, after = (y + NY - 2) % NY, (y + 2) % NY
    for plane in range(2):
        for side, src in enumerate((before, after)):
            ref = kvb.at[src, plane]
            rcopy(ref, ref, s_k.at[0], r_k2.at[side, plane], row_of(1)).wait_recv()
            if side == plane:
                send = rcopy(ref, ref, s_k.at[6 + side], r_k4.at[side], row_of((2, NY - 2)[side]))
                send.start()
                kv_sends.append(send)
            send = rcopy(ref, ref, s_k.at[8 + 2 * side + plane], r_k3.at[side, plane], row_of((1, NY - 1)[side]))
            send.start()
            kv_sends.append(send)

    query_w = (acc4[:, 384:512] * inv).astype(BF16)

    @pl.when(has_prev)
    def _():
        rcopy(wkv, pwkv, s_w, r_w, before_me).wait_recv()

    @pl.when(jnp.logical_not(has_prev))
    def _():
        pwkv[...] = jnp.zeros_like(pwkv)

    prev = pwkv[...]
    keys = jnp.concatenate([prev[:, :64], own_pair[:, :64]], axis=0)
    values = jnp.concatenate([prev[:, 64:], own_pair[:, 64:]], axis=0)
    q_row, k_col = iota((T, 2 * T), 0), iota((T, 2 * T), 1)
    usable = (k_col > q_row) & (k_col <= q_row + T) & ((k_col >= T) | has_prev)
    outs = []
    for h in range(2):
        logit = dot_nt(query_w[:, 64 * h : 64 * h + 64], keys) * (0.125 * LOG2E)
        logit = jnp.where(usable, logit, -jnp.inf)
        sink = sinks_s[h] * LOG2E
        top = jnp.maximum(jnp.max(logit, axis=1, keepdims=True), sink)
        weight = jnp.exp2(logit - top)
        norm = jnp.sum(weight, axis=1, keepdims=True) + jnp.exp2(sink - top)
        outs.append(dot((weight / norm).astype(BF16), values))
    win_out = jnp.concatenate(outs, axis=1).astype(BF16).astype(F32)

    def project_out(result, gain, weight, mix, inbound, buf, dst, slot, ssem, rsem):
        scaled = (result * gain[...]).astype(BF16)
        sums = split(jnp.sum(result * result, axis=1, keepdims=True))
        for core in range(2):
            for chip in range(NX):
                rows = slice(32 * chip + 16 * core, 32 * chip + 16 * core + 16)
                mix[core, 16 * chip : 16 * chip + 16, :128] = scaled[rows]
                mix[core, 16 * chip : 16 * chip + 16, 128:] = sums[rows]
        over = rcopy(mix.at[1 - c], inbound, s_pair.at[2 + slot], r_pair.at[2 + slot], (sp, partner))
        over.start()
        theirs_w = weight.at[1 - c]
        rcopy(theirs_w, theirs_w, s_pair.at[0], r_pair.at[slot], (sp, partner)).wait_recv()
        mine = mix[c, :, :128]
        own = [dot(mine, weight[c, :, n * 512 : n * 512 + 512]) for n in range(4)]
        over.wait_recv()
        theirs = inbound[:, :128]
        for n in range(4):
            part = own[n] + dot(theirs, weight[1 - c, :, n * 512 : n * 512 + 512])
            buf[:, n * 512 : n * 512 + 512] = part.astype(BF16)
        both = mix[c, :, 128:].astype(F32) + inbound[:, 128:].astype(F32)
        buf[:, D:] = split(jnp.sum(both, axis=1, keepdims=True))
        sends = []
        for d in (2, 1, 3):
            to = (x + d) % NX
            rows = buf.at[pl.ds(pl.multiple_of(to * 16, 16), 16), :]
            sends.append(rcopy(rows, dst.at[x], ssem.at[d], rsem.at[x], (sp, to * 2 + c)))
        for send in sends:
            send.start()
        return sends + [over]

    win_sends = project_out(win_out, wg_v, wo_w, mix_b, in_b, bb, rb, 0, s_rb, r_rb)

    def spread(j):
        key_t, val = kvb[j, 0], kvb[j, 1]
        zero = jnp.zeros_like(key_t)
        feat = iota((T, 128), 0) < 64
        kbd[j, :, :T] = jnp.where(feat, key_t, zero)
        kbd[j, :, T:] = jnp.where(feat, zero, key_t)
        lane = iota((T, 128), 1) < 64
        vbd[j, :T, :] = jnp.where(lane, val, zero)
        vbd[j, T:, :] = jnp.where(lane, zero, val)

    bias_row = jnp.where(iota((1, 2 * T), 1) < T, bias_s[0] * LOG2E, bias_s[1] * LOG2E)

    in_head0 = iota((2 * T, 128), 1) < 64
    far = [(y + d) % NY for d in range(NY)]
    query_pairs = (NZ - z + 1) // 2
    early = jnp.minimum(query_pairs, 2)
    units = 4 * query_pairs

    def unit(i):
        at = jnp.clip(i, 0, units - 1)
        mid, rest = at - 2 * early, jnp.maximum(at - 4 * early, 0)
        p = jnp.where(mid < 0, at // 2, jnp.where(mid < 2 * early, early - 1 - mid // 2, early + rest // 4))
        k = jnp.where(mid < 0, at % 2, jnp.where(mid < 2 * early, 2 + mid % 2, rest % 4))
        real = (i >= 0) & (i < units)
        first = jnp.where(k == 0, y, jnp.where(k == 1, after, jnp.where(k == 2, far[1], far[3])))
        second = jnp.where(k == 0, before, jnp.where(k == 1, far[7], jnp.where(k == 2, far[5], far[4])))
        rows = rows_of(jnp.where(real, z + 2 * p, NZ + 1), 2)
        return p, k, real, (first, second), rows

    halves = (pl.ds(0, 2 * T), pl.ds(2 * T, 2 * T))

    def kv_wait(src):
        rcopy(kvb.at[src], kvb.at[src], s_k.at[0], r_k.at[src], row_of(1)).wait_recv()

    def await_queries(p):
        for n in range(2):
            q = z + 2 * p + n

            @pl.when((q > z) & (q < NZ))
            def _(q=q):
                block = qb.at[rows_of(q), :]
                rcopy(block, block, s_q.at[0], r_q.at[q], (q * NY + y, tp)).wait_recv()

    def total_of(q):
        rows = rows_of(q)
        part, total = parts[NY - 1, rows, :], logs[NY - 1, rows, :]
        for j in range(NY - 2, -1, -1):
            part = part + jnp.exp2(-total) * parts[j, rows, :]
            total = total + logs[j, rows, :]
        flipped = total.T
        return part, (flipped[0:1, :], flipped[64:65, :])

    def p_send(to):
        return rcopy(pout.at[to], prec.at[z], s_p.at[to], r_p.at[z], (to * NY + y, tp))

    def l_send(to):
        return rcopy(lout.at[to], lrec.at[z], s_l.at[to], r_l.at[z], (to * NY + y, tp))

    def give(zq):
        part, (l0, l1) = total_of(zq)
        pout[zq] = part.astype(BF16)
        lout[zq, 0:1, :] = l0
        lout[zq, 1:2, :] = l1
        l_send(zq).start()
        p_send(zq).start()

    def unit_step(i, now):
        later = 1 - now
        _, _, _, pair_d, rows_d = unit(i - 4)
        p, _, _, pair, _ = unit(i)
        for half, j in zip(halves, pair_d):
            parts[j, rows_d, :] = dot(weight_b[now, half, :], vbd[j])
        weight_b[later] = jnp.exp2(expo[now]).astype(BF16)
        expo[later] = diff[now] - dot(soft_b[now], tri[...])
        _, _, _, pair_b, rows_b = unit(i - 1)
        for half, j in zip(halves, pair_b):
            score = raw[now, half, :] + bias_row
            soft = jnp.maximum(score, jnp.log(1.0 + jnp.exp2(jnp.minimum(score, 126.0))) * LOG2E)
            diff[later, half, :] = score - soft
            soft_b[later, half, :] = soft.astype(BF16)
            sum0 = jnp.sum(soft[:, :T], axis=1, keepdims=True)
            sum1 = jnp.sum(soft[:, T:], axis=1, keepdims=True)
            logs[j, rows_b, :] = jnp.where(in_head0, sum0, sum1)
        own_rows = rows_of(jnp.minimum(z + 2 * p, NZ - 1), 2)
        for half, j in zip(halves, pair):
            score = dot(qb[own_rows, :], kbd[j])
            limit = jnp.where(p == 0, (y - j) * T, NY * T)
            raw[later, pl.ds(half.start, T), :] = jnp.where(offset[...] < limit, score[:T], -1e30)
            raw[later, pl.ds(half.start + T, T), :] = score[T:]

    def give_done(i):
        p_d, k_d, real_d, _, _ = unit(i)
        for n in range(2):
            q_d = z + 2 * p_d + n

            @pl.when(real_d & (k_d == 3) & (q_d > z) & (q_d < NZ))
            def _(q_d=q_d):
                give(q_d)

    def two_steps(i, _):
        first = 2 * i
        p, k, _, _, _ = unit(first)

        @pl.when((k == 0) & (first < units))
        def _():
            await_queries(p)

        @pl.when(i == 0)
        def _():
            kv_wait(far[7])
            spread(far[7])

        @pl.when(i == early)
        def _():
            kv_wait(far[1])
            spread(far[1])
            for side, src in enumerate((far[5], far[3])):
                for plane in range(2):
                    ref = kvb.at[src, plane]
                    rcopy(ref, ref, s_k.at[0], r_k3.at[side, plane], row_of(1)).wait_recv()
                spread(src)
            for n in range(2):
                rcopy(kvb.at[far[4], n], kvb.at[far[4], n], s_k.at[0], r_k4.at[n], row_of(1)).wait_recv()
            spread(far[4])

        unit_step(first, 0)
        unit_step(first + 1, 1)
        give_done(first - 3)
        return 0

    spread(y)
    spread(before)
    spread(after)
    lax.fori_loop(0, 2 * query_pairs + 2, two_steps, 0)

    own_part, own_logs = total_of(z)

    def factor_of(rows):
        spread_rows = [jnp.broadcast_to(jnp.exp2(-row), (64, 128)) for row in rows]
        return jnp.concatenate(spread_rows, axis=0).T

    acc_p[...] = jnp.zeros_like(acc_p)

    def merge(src, _):
        rcopy(lout.at[src], lrec.at[src], s_l.at[0], r_l.at[src], (src * NY + y, tp)).wait_recv()
        factor = factor_of((lrec[src, 0:1, :], lrec[src, 1:2, :]))
        rcopy(pout.at[src], prec.at[src], s_p.at[0], r_p.at[src], (src * NY + y, tp)).wait_recv()
        acc_p[...] = prec[src].astype(F32) + factor * acc_p[...]
        return 0

    lax.fori_loop(0, z, merge, 0)
    acc_p[...] = own_part + factor_of(own_logs) * acc_p[...]

    stick_out = acc_p[...].astype(BF16).astype(F32)
    stick_sends = project_out(stick_out, sg_v, wo_s, mix_a, in_a, ab, ra, 1, s_ra, r_ra)

    def gathered(buf, dst, rsem):
        total = buf[pl.ds(pl.multiple_of(x * 16, 16), 16), :].astype(F32)
        for d in (1, 3, 2):
            src = (x + d) % NX
            rcopy(dst.at[src], dst.at[src], s_ra.at[0], rsem.at[src], (sp, src * 2 + c)).wait_recv()
            total = total + dst[src].astype(F32)
        scale = lax.rsqrt(jnp.sum(total[:, D:], axis=1, keepdims=True) * (1.0 / 1024) + EPS)
        return total[:, :D] * scale

    combined = gathered(bb, rb, r_rb)
    combined = combined + gathered(ab, ra, r_ra)
    mean = jnp.sum(combined * combined, axis=1, keepdims=True) * (1.0 / D)
    out[...] = (combined * lax.rsqrt(mean + EPS) * post_v[...]).astype(BF16)

    for send in tok_sends + kv_sends + pair_sends + win_sends + stick_sends:
        send.wait_send()

    @pl.when(has_next)
    def _():
        win_send.wait_send()

    for n in (4, 5, 6):
        rcopy(own_tok, own_tok, s_a.at[n], r_a.at[tp], (sp, partner)).wait_send()

    def q_drain(i, _):
        q_send(i).wait_send()
        return 0

    lax.fori_loop(0, z, q_drain, 0)

    def p_drain(i, _):
        p_send(NZ - 1 - i).wait_send()
        l_send(NZ - 1 - i).wait_send()
        return 0

    lax.fori_loop(0, NZ - 1 - z, p_drain, 0)


def shards(
    tokens, pre_gain, w_query_stick, w_key_stick, w_value_stick, w_query_window, w_key_window, w_value_window,
    stick_bias, sinks, stick_gain, window_gain, w_out_stick, w_out_window, post_gain,
):
    anywhere = pl.BlockSpec(memory_space=pl.ANY)
    dma = pltpu.SemaphoreType.DMA
    vm = pltpu.VMEM
    scratch = [
        vm((NTP, T, CH), BF16), vm((D, 512), BF16), vm((128, D), BF16),
        vm((2, 128, D), BF16), vm((2, 128, D), BF16), vm((1, D), F32), vm((1, 128), F32), vm((1, 128), F32), vm((1, D), F32),
        vm((T, 512), F32), vm((T, 128), F32), vm((T, 128), F32),
        vm((NY, 2, T, 128), BF16), vm(((NZ + 1) * T, 128), BF16), vm((NY, 128, 2 * T), BF16), vm((NY, 2 * T, 128), BF16),
        vm((256, 256), BF16), vm((2, 4 * T, 2 * T), F32), vm((2, 4 * T, 2 * T), BF16), vm((2, 4 * T, 2 * T), F32),
        vm((2, 4 * T, 2 * T), F32), vm((2, 4 * T, 2 * T), BF16),
        vm((NY, (NZ + 3) * T, 128), F32), vm((NY, (NZ + 3) * T, 128), F32), vm((T, 2 * T), jnp.int32),
        vm((T, 128), BF16), vm((T, 128), BF16), vm((NZ, T, 128), BF16), vm((NZ, T, 128), BF16),
        vm((NZ, 2, 128), F32), vm((NZ, 2, 128), F32),
        vm((T, 128), F32), vm((64, PACK), BF16), vm((64, PACK), BF16),
        vm((NX, 16, PACK), BF16), vm((NX, 16, PACK), BF16), vm((2, 64, 256), BF16), vm((2, 64, 256), BF16),
        vm((64, 256), BF16), vm((64, 256), BF16), pltpu.SMEM((2,), F32), pltpu.SMEM((2,), F32),
        dma((15,)), dma((7,)), dma((NTP,)), dma((12,)), dma((NY,)), dma((2, 2)), dma((2, 2)), dma((2,)), dma((NZ,)), dma((NZ,)), dma, dma, pltpu.SemaphoreType.REGULAR,
        dma((NZ,)), dma((NZ,)), dma((NZ,)), dma((NZ,)), dma((NX,)), dma((NX,)), dma((NX,)), dma((NX,)), dma((4,)), dma((4,)),
    ]
    return pl.pallas_call(
        kernel,
        out_shape=jax.ShapeDtypeStruct((T // NTP, D), BF16),
        in_specs=[anywhere] * 15,
        out_specs=pl.BlockSpec(memory_space=pltpu.VMEM),
        scratch_shapes=scratch,
        compiler_params=pltpu.CompilerParams(
            collective_id=0, has_side_effects=True, vmem_limit_bytes=60 * 1024 * 1024
        ),
    )(
        tokens, pre_gain.reshape(1, -1), w_query_stick, w_key_stick, w_value_stick, w_query_window,
        w_key_window.T, w_value_window.T, stick_bias, sinks, stick_gain.reshape(1, -1), window_gain.reshape(1, -1),
        w_out_stick, w_out_window, post_gain.reshape(1, -1),
    )


def solution(mesh):
    in_specs = (
        P("sp", "tp"),
        P(),
        P(None, "tp"),
        P(None, "tp"),
        P(None, "tp"),
        P(None, "tp"),
        P(None, "tp"),
        P(None, "tp"),
        P("tp"),
        P("tp"),
        P("tp"),
        P("tp"),
        P("tp", None),
        P("tp", None),
        P(),
    )
    out_specs = P(("sp", "tp"), None)
    return jax.shard_map(shards, mesh=mesh, in_specs=in_specs, out_specs=out_specs, check_vma=False)
```

```python
import functools

import jax
import jax.numpy as jnp
from jax import lax
from jax.experimental import pallas as pl
from jax.experimental.pallas import tpu as pltpu
from jax.sharding import PartitionSpec as P

T = 128
D = 2048
CH = 256
NY = 8
NZ = 8
NTP = 8
NX = 4
LOG2E = 1.4426950408889634
EPS = 1e-06
PACK = D + 128
MESH = pl.DeviceIdType.MESH
F32 = jnp.float32
BF16 = jnp.bfloat16


def dot(a, b):
    return jnp.dot(a, b, preferred_element_type=F32)


def dot_nt(a, b):
    return lax.dot_general(a, b, (((1,), (1,)), ((), ())), preferred_element_type=F32)


def iota(shape, dim):
    return lax.broadcasted_iota(jnp.int32, shape, dim)


def split(total):
    high = total.astype(BF16).astype(F32)
    lane = iota((total.shape[0], 128), 1)
    return jnp.where(lane == 0, high, jnp.where(lane == 1, total - high, 0.0)).astype(BF16)


def kernel(
    tok, pre, wqs, wks, wvs, wqw, wkw, wvw, bias, sinks, sgain, wgain, wos, wow, post,
    out,
    tok_all, w4, w_win, wo_s, wo_w, pre_v, sg_v, wg_v, post_v,
    acc4, acc_w, sq, kvb, qb, kbd, vbd, tri, raw, soft_b, diff, expo, weight_b, parts, logs, offset,
    wkv, pwkv, pout, prec, lout, lrec, acc_p, ab, bb, ra, rb, mix_a, mix_b, in_a, in_b, bias_s, sinks_s,
    lsem, s_a, r_a, s_k, r_k, r_k2, r_k3, r_k4, s_q, r_q, s_w, r_w, ready, s_p, r_p, s_l, r_l, s_ra, r_ra, s_rb, r_rb,
    s_pair, r_pair,
):
    sp = lax.axis_index("sp")
    tp = lax.axis_index("tp")
    z = sp // NY
    y = sp % NY
    x = tp // 2
    c = tp % 2

    def rcopy(src, dst, ssem, rsem, dev):
        return pltpu.make_async_remote_copy(
            src_ref=src, dst_ref=dst, send_sem=ssem, recv_sem=rsem, device_id=dev, device_id_type=MESH
        )

    def rows_of(block, count=1):
        return pl.ds(pl.multiple_of(block * T, T), count * T)

    loads = [pltpu.make_async_copy(tok, tok_all.at[tp], lsem.at[0])]
    pairs = [
        (pre, pre_v), (wks, w4.at[:, pl.ds(0, 128)]), (wvs, w4.at[:, pl.ds(128, 128)]),
        (wqs, w4.at[:, pl.ds(256, 128)]), (wqw, w4.at[:, pl.ds(384, 128)]),
        (wkw, w_win.at[pl.ds(0, 64), :]), (wvw, w_win.at[pl.ds(64, 64), :]),
        (bias, bias_s), (sinks, sinks_s), (sgain, sg_v), (wgain, wg_v), (post, post_v), (wos, wo_s.at[c]), (wow, wo_w.at[c]),
    ]
    for n, (src, dst) in enumerate(pairs):
        loads.append(pltpu.make_async_copy(src, dst, lsem.at[n + 1]))
    for load in loads:
        load.start()

    barrier = pltpu.get_barrier_semaphore()

    def greet(dev):
        pl.semaphore_signal(barrier, inc=1, device_id=dev, device_id_type=MESH)

    greeted = [(sp, (tp + d) % NTP) for d in range(1, NTP)]
    greeted += [(z * NY + (y + d) % NY, tp) for d in (1, 2, NY - 2, NY - 1)]
    for dev in greeted:
        greet(dev)

    def greet_row(i, _):
        greet((i * NY + y, tp))
        return 0

    lax.fori_loop(z + 1, NZ, greet_row, 0)
    has_next = sp < NY * NZ - 1
    has_prev = sp > 0
    starts_row = (y == 0) & has_prev
    ends_row = (y == NY - 1) & has_next
    nxt = ((sp + 1) % (NY * NZ), tp)
    before_me = ((sp + NY * NZ - 1) % (NY * NZ), tp)

    @pl.when(ends_row)
    def _():
        greet(nxt)

    row2, col2 = iota((256, 256), 0), iota((256, 256), 1)
    tri[...] = jnp.where((row2 > col2) & (row2 // T == col2 // T), 1.0, 0.0).astype(BF16)
    offset[...] = iota((T, 2 * T), 1) % T - iota((T, 2 * T), 0)
    acc4[...] = jnp.zeros_like(acc4)
    acc_w[...] = jnp.zeros_like(acc_w)
    sq[...] = jnp.zeros_like(sq)
    for ref in (raw, soft_b, diff, expo, weight_b):
        ref[...] = jnp.zeros_like(ref)
    qb[NZ * T :, :] = jnp.zeros((T, 128), BF16)

    pl.semaphore_wait(barrier, len(greeted) + z + jnp.where(starts_row, 1, 0))

    @pl.when(starts_row)
    def _():
        pl.semaphore_signal(ready, inc=1, device_id=before_me, device_id_type=MESH)

    loads[0].wait()

    partner = x * 2 + (1 - c)
    own_tok = tok_all.at[tp]
    tok_sends = []
    for n, d in enumerate((2, 1, 3)):
        peer = ((x + d) % NX) * 2 + c
        tok_sends.append(rcopy(own_tok, own_tok, s_a.at[n], r_a.at[tp], (sp, peer)))
    tok_sends.append(rcopy(own_tok, own_tok, s_a.at[3], r_a.at[tp], (sp, partner)))
    for send in tok_sends:
        send.start()
    for load in loads[1:8]:
        load.wait()

    def feature_step(i, _):
        dist = jnp.where(i < 2, 0, jnp.where((i == 2) | (i == 5), 1, jnp.where((i == 3) | (i == 6), 3, 2)))
        core = jnp.where((i == 1) | (i >= 5), 1 - c, c)
        src = ((x + dist) % NX) * 2 + core
        block = tok_all.at[src]

        @pl.when(i > 0)
        def _():
            rcopy(block, block, s_a.at[0], r_a.at[src], (sp, partner)).wait_recv()

        @pl.when((i >= 2) & (i <= 4))
        def _():
            rcopy(block, block, s_a.at[i + 2], r_a.at[src], (sp, partner)).start()

        feats = block[...].astype(F32)
        sq[...] += feats[:, :128] * feats[:, :128] + feats[:, 128:] * feats[:, 128:]
        at = pl.ds(pl.multiple_of(src * CH, CH), CH)
        scaled = (feats * pre_v[:, at]).astype(BF16)
        acc4[...] += dot(scaled, w4[at, :])
        acc_w[...] += dot_nt(scaled, w_win[:, at])
        return 0

    lax.fori_loop(0, NTP, feature_step, 0)
    inv = lax.rsqrt(jnp.sum(sq[...], axis=1, keepdims=True) * (1.0 / D) + EPS)

    kvb[y, 0] = (acc4[:, 0:128] * inv).T.astype(BF16)
    kvb[y, 1] = (acc4[:, 128:256] * inv).astype(BF16)
    own_kv = kvb.at[y]
    row_of = lambda d: (z * NY + (y + d) % NY, tp)
    kv_sends = []
    for plane in range(2):
        for side, d in enumerate((2, NY - 2)):
            ref = kvb.at[y, plane]
            kv_sends.append(rcopy(ref, ref, s_k.at[2 * plane + side], r_k2.at[side, plane], row_of(d)))
    for send in kv_sends:
        send.start()
    qb[rows_of(z), :] = (acc4[:, 256:384] * (inv * (0.125 * LOG2E))).astype(BF16)

    def q_send(i):
        return rcopy(qb.at[rows_of(z), :], qb.at[rows_of(z), :], s_q.at[i], r_q.at[z], (i * NY + y, tp))

    def q_start(i, _):
        q_send(i).start()
        return 0

    lax.fori_loop(0, z, q_start, 0)

    own_pair = (acc_w[...] * inv).astype(BF16)
    wkv[...] = own_pair

    @pl.when(ends_row)
    def _():
        pl.semaphore_wait(ready, 1)

    win_send = rcopy(wkv, pwkv, s_w, r_w, nxt)

    @pl.when(has_next)
    def _():
        win_send.start()

    for n, d in enumerate((1, NY - 1)):
        send = rcopy(own_kv, own_kv, s_k.at[4 + n], r_k.at[y], row_of(d))
        send.start()
        kv_sends.append(send)
    for load in loads[8:]:
        load.wait()
    pair_sends = []
    for n, ref in enumerate((wo_w.at[c], wo_s.at[c])):
        pair_sends.append(rcopy(ref, ref, s_pair.at[n], r_pair.at[n], (sp, partner)))
    for send in pair_sends:
        send.start()

    before, after = (y + NY - 2) % NY, (y + 2) % NY
    for plane in range(2):
        for side, src in enumerate((before, after)):
            ref = kvb.at[src, plane]
            rcopy(ref, ref, s_k.at[0], r_k2.at[side, plane], row_of(1)).wait_recv()
            if side == plane:
                send = rcopy(ref, ref, s_k.at[6 + side], r_k4.at[side], row_of((2, NY - 2)[side]))
                send.start()
                kv_sends.append(send)
            send = rcopy(ref, ref, s_k.at[8 + 2 * side + plane], r_k3.at[side, plane], row_of((1, NY - 1)[side]))
            send.start()
            kv_sends.append(send)

    query_w = (acc4[:, 384:512] * inv).astype(BF16)

    @pl.when(has_prev)
    def _():
        rcopy(wkv, pwkv, s_w, r_w, before_me).wait_recv()

    @pl.when(jnp.logical_not(has_prev))
    def _():
        pwkv[...] = jnp.zeros_like(pwkv)

    prev = pwkv[...]
    keys = jnp.concatenate([prev[:, :64], own_pair[:, :64]], axis=0)
    values = jnp.concatenate([prev[:, 64:], own_pair[:, 64:]], axis=0)
    q_row, k_col = iota((T, 2 * T), 0), iota((T, 2 * T), 1)
    usable = (k_col > q_row) & (k_col <= q_row + T) & ((k_col >= T) | has_prev)
    outs = []
    for h in range(2):
        logit = dot_nt(query_w[:, 64 * h : 64 * h + 64], keys) * (0.125 * LOG2E)
        logit = jnp.where(usable, logit, -jnp.inf)
        sink = sinks_s[h] * LOG2E
        top = jnp.maximum(jnp.max(logit, axis=1, keepdims=True), sink)
        weight = jnp.exp2(logit - top)
        norm = jnp.sum(weight, axis=1, keepdims=True) + jnp.exp2(sink - top)
        outs.append(dot((weight / norm).astype(BF16), values))
    win_out = jnp.concatenate(outs, axis=1).astype(BF16).astype(F32)

    def project_out(result, gain, weight, mix, inbound, buf, dst, slot, ssem, rsem):
        scaled = (result * gain[...]).astype(BF16)
        sums = split(jnp.sum(result * result, axis=1, keepdims=True))
        for core in range(2):
            for chip in range(NX):
                rows = slice(32 * chip + 16 * core, 32 * chip + 16 * core + 16)
                mix[core, 16 * chip : 16 * chip + 16, :128] = scaled[rows]
                mix[core, 16 * chip : 16 * chip + 16, 128:] = sums[rows]
        over = rcopy(mix.at[1 - c], inbound, s_pair.at[2 + slot], r_pair.at[2 + slot], (sp, partner))
        over.start()
        theirs_w = weight.at[1 - c]
        rcopy(theirs_w, theirs_w, s_pair.at[0], r_pair.at[slot], (sp, partner)).wait_recv()
        mine = mix[c, :, :128]
        own = [dot(mine, weight[c, :, n * 512 : n * 512 + 512]) for n in range(4)]
        over.wait_recv()
        theirs = inbound[:, :128]
        for n in range(4):
            part = own[n] + dot(theirs, weight[1 - c, :, n * 512 : n * 512 + 512])
            buf[:, n * 512 : n * 512 + 512] = part.astype(BF16)
        both = mix[c, :, 128:].astype(F32) + inbound[:, 128:].astype(F32)
        buf[:, D:] = split(jnp.sum(both, axis=1, keepdims=True))
        sends = []
        for d in (2, 1, 3):
            to = (x + d) % NX
            rows = buf.at[pl.ds(pl.multiple_of(to * 16, 16), 16), :]
            sends.append(rcopy(rows, dst.at[x], ssem.at[d], rsem.at[x], (sp, to * 2 + c)))
        for send in sends:
            send.start()
        return sends + [over]

    win_sends = project_out(win_out, wg_v, wo_w, mix_b, in_b, bb, rb, 0, s_rb, r_rb)

    def spread(j):
        key_t, val = kvb[j, 0], kvb[j, 1]
        zero = jnp.zeros_like(key_t)
        feat = iota((T, 128), 0) < 64
        kbd[j, :, :T] = jnp.where(feat, key_t, zero)
        kbd[j, :, T:] = jnp.where(feat, zero, key_t)
        lane = iota((T, 128), 1) < 64
        vbd[j, :T, :] = jnp.where(lane, val, zero)
        vbd[j, T:, :] = jnp.where(lane, zero, val)

    bias_row = jnp.where(iota((1, 2 * T), 1) < T, bias_s[0] * LOG2E, bias_s[1] * LOG2E)

    in_head0 = iota((2 * T, 128), 1) < 64
    far = [(y + d) % NY for d in range(NY)]
    query_pairs = (NZ - z + 1) // 2
    early = jnp.minimum(query_pairs, 2)
    units = 4 * query_pairs

    def unit(i):
        at = jnp.clip(i, 0, units - 1)
        mid, rest = at - 2 * early, jnp.maximum(at - 4 * early, 0)
        turn = jnp.where(z == 3, mid // 2, early - 1 - mid // 2)
        p = jnp.where(mid < 0, at // 2, jnp.where(mid < 2 * early, turn, early + rest // 4))
        k = jnp.where(mid < 0, at % 2, jnp.where(mid < 2 * early, 2 + mid % 2, rest % 4))
        real = (i >= 0) & (i < units)
        first = jnp.where(k == 0, y, jnp.where(k == 1, after, jnp.where(k == 2, far[1], far[3])))
        second = jnp.where(k == 0, before, jnp.where(k == 1, far[7], jnp.where(k == 2, far[5], far[4])))
        rows = rows_of(jnp.where(real, z + 2 * p, NZ + 1), 2)
        return p, k, real, (first, second), rows

    halves = (pl.ds(0, 2 * T), pl.ds(2 * T, 2 * T))

    def kv_wait(src):
        rcopy(kvb.at[src], kvb.at[src], s_k.at[0], r_k.at[src], row_of(1)).wait_recv()

    def await_queries(p):
        for n in range(2):
            q = z + 2 * p + n

            @pl.when((q > z) & (q < NZ))
            def _(q=q):
                block = qb.at[rows_of(q), :]
                rcopy(block, block, s_q.at[0], r_q.at[q], (q * NY + y, tp)).wait_recv()

    def total_of(q):
        rows = rows_of(q)
        part, total = parts[NY - 1, rows, :], logs[NY - 1, rows, :]
        for j in range(NY - 2, -1, -1):
            part = part + jnp.exp2(-total) * parts[j, rows, :]
            total = total + logs[j, rows, :]
        flipped = total.T
        return part, (flipped[0:1, :], flipped[64:65, :])

    def p_send(to):
        return rcopy(pout.at[to], prec.at[z], s_p.at[to], r_p.at[z], (to * NY + y, tp))

    def l_send(to):
        return rcopy(lout.at[to], lrec.at[z], s_l.at[to], r_l.at[z], (to * NY + y, tp))

    def give(zq):
        part, (l0, l1) = total_of(zq)
        pout[zq] = part.astype(BF16)
        lout[zq, 0:1, :] = l0
        lout[zq, 1:2, :] = l1
        l_send(zq).start()
        p_send(zq).start()

    def unit_step(i, now, stages=5):
        later = 1 - now
        _, _, _, pair_d, rows_d = unit(i - 4)
        for half, j in zip(halves, pair_d):
            parts[j, rows_d, :] = dot(weight_b[now, half, :], vbd[j])
        if stages >= 2:
            weight_b[later] = jnp.exp2(expo[now]).astype(BF16)
        if stages >= 3:
            expo[later] = diff[now] - dot(soft_b[now], tri[...])
        if stages >= 4:
            _, _, _, pair_b, rows_b = unit(i - 1)
            for half, j in zip(halves, pair_b):
                score = raw[now, half, :] + bias_row
                soft = jnp.maximum(score, jnp.log(1.0 + jnp.exp2(jnp.minimum(score, 126.0))) * LOG2E)
                diff[later, half, :] = score - soft
                soft_b[later, half, :] = soft.astype(BF16)
                sum0 = jnp.sum(soft[:, :T], axis=1, keepdims=True)
                sum1 = jnp.sum(soft[:, T:], axis=1, keepdims=True)
                logs[j, rows_b, :] = jnp.where(in_head0, sum0, sum1)
        if stages >= 5:
            p, _, _, pair, _ = unit(i)
            own_rows = rows_of(jnp.minimum(z + 2 * p, NZ - 1), 2)
            limit_of = lambda j: jnp.where(p == 0, (y - j) * T, NY * T)
            for half, j in zip(halves, pair):
                score = dot(qb[own_rows, :], kbd[j])
                raw[later, pl.ds(half.start, T), :] = jnp.where(offset[...] < limit_of(j), score[:T], -1e30)
                raw[later, pl.ds(half.start + T, T), :] = score[T:]

    def give_done(i):
        p_d, k_d, real_d, _, _ = unit(i)
        for n in range(2):
            q_d = z + 2 * p_d + n

            @pl.when(real_d & (k_d == 3) & (q_d > z) & (q_d < NZ))
            def _(q_d=q_d):
                give(q_d)

    def two_steps(i, _):
        first = 2 * i
        p, k, _, _, _ = unit(first)

        @pl.when((k == 0) & (first < units))
        def _():
            await_queries(p)

        @pl.when(i == 0)
        def _():
            kv_wait(far[7])
            spread(far[7])

        @pl.when(i == early)
        def _():
            kv_wait(far[1])
            spread(far[1])
            for side, src in enumerate((far[5], far[3])):
                for plane in range(2):
                    ref = kvb.at[src, plane]
                    rcopy(ref, ref, s_k.at[0], r_k3.at[side, plane], row_of(1)).wait_recv()
                spread(src)
            for n in range(2):
                rcopy(kvb.at[far[4], n], kvb.at[far[4], n], s_k.at[0], r_k4.at[n], row_of(1)).wait_recv()
            spread(far[4])

        unit_step(first, 0)
        unit_step(first + 1, 1)
        give_done(first - 3)
        return 0

    spread(y)
    spread(before)
    spread(after)
    lax.fori_loop(0, 2 * query_pairs, two_steps, 0)
    unit_step(units, 0, 4)
    unit_step(units + 1, 1, 3)
    give_done(units - 3)
    unit_step(units + 2, 0, 2)
    unit_step(units + 3, 1, 1)
    give_done(units - 1)

    own_part, own_logs = total_of(z)

    def factor_of(rows):
        spread_rows = [jnp.broadcast_to(jnp.exp2(-row), (64, 128)) for row in rows]
        return jnp.concatenate(spread_rows, axis=0).T

    acc_p[...] = jnp.zeros_like(acc_p)

    def merge(src, _):
        rcopy(lout.at[src], lrec.at[src], s_l.at[0], r_l.at[src], (src * NY + y, tp)).wait_recv()
        factor = factor_of((lrec[src, 0:1, :], lrec[src, 1:2, :]))
        rcopy(pout.at[src], prec.at[src], s_p.at[0], r_p.at[src], (src * NY + y, tp)).wait_recv()
        acc_p[...] = prec[src].astype(F32) + factor * acc_p[...]
        return 0

    lax.fori_loop(0, z, merge, 0)
    acc_p[...] = own_part + factor_of(own_logs) * acc_p[...]

    stick_out = acc_p[...].astype(BF16).astype(F32)
    stick_sends = project_out(stick_out, sg_v, wo_s, mix_a, in_a, ab, ra, 1, s_ra, r_ra)

    def gathered(buf, dst, rsem):
        total = buf[pl.ds(pl.multiple_of(x * 16, 16), 16), :].astype(F32)
        for d in (1, 3, 2):
            src = (x + d) % NX
            rcopy(dst.at[src], dst.at[src], s_ra.at[0], rsem.at[src], (sp, src * 2 + c)).wait_recv()
            total = total + dst[src].astype(F32)
        scale = lax.rsqrt(jnp.sum(total[:, D:], axis=1, keepdims=True) * (1.0 / 1024) + EPS)
        return total[:, :D] * scale

    combined = gathered(bb, rb, r_rb)
    combined = combined + gathered(ab, ra, r_ra)
    mean = jnp.sum(combined * combined, axis=1, keepdims=True) * (1.0 / D)
    out[...] = (combined * lax.rsqrt(mean + EPS) * post_v[...]).astype(BF16)

    for send in tok_sends + kv_sends + pair_sends + win_sends + stick_sends:
        send.wait_send()

    @pl.when(has_next)
    def _():
        win_send.wait_send()

    for n in (4, 5, 6):
        rcopy(own_tok, own_tok, s_a.at[n], r_a.at[tp], (sp, partner)).wait_send()

    def q_drain(i, _):
        q_send(i).wait_send()
        return 0

    lax.fori_loop(0, z, q_drain, 0)

    def p_drain(i, _):
        p_send(NZ - 1 - i).wait_send()
        l_send(NZ - 1 - i).wait_send()
        return 0

    lax.fori_loop(0, NZ - 1 - z, p_drain, 0)


def shards(
    tokens, pre_gain, w_query_stick, w_key_stick, w_value_stick, w_query_window, w_key_window, w_value_window,
    stick_bias, sinks, stick_gain, window_gain, w_out_stick, w_out_window, post_gain,
):
    anywhere = pl.BlockSpec(memory_space=pl.ANY)
    dma = pltpu.SemaphoreType.DMA
    vm = pltpu.VMEM
    scratch = [
        vm((NTP, T, CH), BF16), vm((D, 512), BF16), vm((128, D), BF16),
        vm((2, 128, D), BF16), vm((2, 128, D), BF16), vm((1, D), F32), vm((1, 128), F32), vm((1, 128), F32), vm((1, D), F32),
        vm((T, 512), F32), vm((T, 128), F32), vm((T, 128), F32),
        vm((NY, 2, T, 128), BF16), vm(((NZ + 1) * T, 128), BF16), vm((NY, 128, 2 * T), BF16), vm((NY, 2 * T, 128), BF16),
        vm((256, 256), BF16), vm((2, 4 * T, 2 * T), F32), vm((2, 4 * T, 2 * T), BF16), vm((2, 4 * T, 2 * T), F32),
        vm((2, 4 * T, 2 * T), F32), vm((2, 4 * T, 2 * T), BF16),
        vm((NY, (NZ + 3) * T, 128), F32), vm((NY, (NZ + 3) * T, 128), F32), vm((T, 2 * T), jnp.int32),
        vm((T, 128), BF16), vm((T, 128), BF16), vm((NZ, T, 128), BF16), vm((NZ, T, 128), BF16),
        vm((NZ, 2, 128), F32), vm((NZ, 2, 128), F32),
        vm((T, 128), F32), vm((64, PACK), BF16), vm((64, PACK), BF16),
        vm((NX, 16, PACK), BF16), vm((NX, 16, PACK), BF16), vm((2, 64, 256), BF16), vm((2, 64, 256), BF16),
        vm((64, 256), BF16), vm((64, 256), BF16), pltpu.SMEM((2,), F32), pltpu.SMEM((2,), F32),
        dma((15,)), dma((7,)), dma((NTP,)), dma((12,)), dma((NY,)), dma((2, 2)), dma((2, 2)), dma((2,)), dma((NZ,)), dma((NZ,)), dma, dma, pltpu.SemaphoreType.REGULAR,
        dma((NZ,)), dma((NZ,)), dma((NZ,)), dma((NZ,)), dma((NX,)), dma((NX,)), dma((NX,)), dma((NX,)), dma((4,)), dma((4,)),
    ]
    return pl.pallas_call(
        kernel,
        out_shape=jax.ShapeDtypeStruct((T // NTP, D), BF16),
        in_specs=[anywhere] * 15,
        out_specs=pl.BlockSpec(memory_space=pltpu.VMEM),
        scratch_shapes=scratch,
        compiler_params=pltpu.CompilerParams(
            collective_id=0, has_side_effects=True, vmem_limit_bytes=60 * 1024 * 1024
        ),
    )(
        tokens, pre_gain.reshape(1, -1), w_query_stick, w_key_stick, w_value_stick, w_query_window,
        w_key_window.T, w_value_window.T, stick_bias, sinks, stick_gain.reshape(1, -1), window_gain.reshape(1, -1),
        w_out_stick, w_out_window, post_gain.reshape(1, -1),
    )


def solution(mesh):
    in_specs = (
        P("sp", "tp"),
        P(),
        P(None, "tp"),
        P(None, "tp"),
        P(None, "tp"),
        P(None, "tp"),
        P(None, "tp"),
        P(None, "tp"),
        P("tp"),
        P("tp"),
        P("tp"),
        P("tp"),
        P("tp", None),
        P("tp", None),
        P(),
    )
    out_specs = P(("sp", "tp"), None)
    return jax.shard_map(shards, mesh=mesh, in_specs=in_specs, out_specs=out_specs, check_vma=False)
```

```python
import functools

import jax
import jax.numpy as jnp
from jax import lax
from jax.experimental import pallas as pl
from jax.experimental.pallas import tpu as pltpu
from jax.sharding import PartitionSpec as P

T = 128
D = 2048
CH = 256
NY = 8
NZ = 8
NTP = 8
NX = 4
LOG2E = 1.4426950408889634
EPS = 1e-06
PACK = D + 128
MESH = pl.DeviceIdType.MESH
F32 = jnp.float32
BF16 = jnp.bfloat16


def dot(a, b):
    return jnp.dot(a, b, preferred_element_type=F32)


def dot_nt(a, b):
    return lax.dot_general(a, b, (((1,), (1,)), ((), ())), preferred_element_type=F32)


def iota(shape, dim):
    return lax.broadcasted_iota(jnp.int32, shape, dim)


def split(total):
    high = total.astype(BF16).astype(F32)
    lane = iota((total.shape[0], 128), 1)
    return jnp.where(lane == 0, high, jnp.where(lane == 1, total - high, 0.0)).astype(BF16)


def kernel(
    tok, pre, wqs, wks, wvs, wqw, wkw, wvw, bias, sinks, sgain, wgain, wos, wow, post,
    out,
    tok_all, w4, w_win, wo_s, wo_w, pre_v, sg_v, wg_v, post_v,
    acc4, acc_w, sq, kvb, qb, kbd, vbd, tri, raw, soft_b, diff, expo, weight_b, parts, logs, offset,
    wkv, pwkv, pout, prec, lout, lrec, acc_p, ab, bb, ra, rb, mix_a, mix_b, in_a, in_b, bias_s, sinks_s,
    lsem, s_a, r_a, s_k, r_k, r_k2, r_k3, r_k4, s_q, r_q, s_w, r_w, ready, s_p, r_p, s_l, r_l, s_ra, r_ra, s_rb, r_rb,
    s_pair, r_pair,
):
    sp = lax.axis_index("sp")
    tp = lax.axis_index("tp")
    z = sp // NY
    y = sp % NY
    x = tp // 2
    c = tp % 2

    def rcopy(src, dst, ssem, rsem, dev):
        return pltpu.make_async_remote_copy(
            src_ref=src, dst_ref=dst, send_sem=ssem, recv_sem=rsem, device_id=dev, device_id_type=MESH
        )

    def rows_of(block, count=1):
        return pl.ds(pl.multiple_of(block * T, T), count * T)

    loads = [pltpu.make_async_copy(tok, tok_all.at[tp], lsem.at[0])]
    pairs = [
        (pre, pre_v), (wks, w4.at[:, pl.ds(0, 128)]), (wvs, w4.at[:, pl.ds(128, 128)]),
        (wqs, w4.at[:, pl.ds(256, 128)]), (wqw, w4.at[:, pl.ds(384, 128)]),
        (wkw, w_win.at[pl.ds(0, 64), :]), (wvw, w_win.at[pl.ds(64, 64), :]),
        (bias, bias_s), (sinks, sinks_s), (sgain, sg_v), (wgain, wg_v), (post, post_v), (wos, wo_s.at[c]), (wow, wo_w.at[c]),
    ]
    for n, (src, dst) in enumerate(pairs):
        loads.append(pltpu.make_async_copy(src, dst, lsem.at[n + 1]))
    for load in loads:
        load.start()

    barrier = pltpu.get_barrier_semaphore()

    def greet(dev):
        pl.semaphore_signal(barrier, inc=1, device_id=dev, device_id_type=MESH)

    greeted = [(sp, (tp + d) % NTP) for d in range(1, NTP)]
    greeted += [(z * NY + (y + d) % NY, tp) for d in (1, 2, NY - 2, NY - 1)]
    for dev in greeted:
        greet(dev)

    def greet_row(i, _):
        greet((i * NY + y, tp))
        return 0

    lax.fori_loop(z + 1, NZ, greet_row, 0)
    has_next = sp < NY * NZ - 1
    has_prev = sp > 0
    starts_row = (y == 0) & has_prev
    ends_row = (y == NY - 1) & has_next
    nxt = ((sp + 1) % (NY * NZ), tp)
    before_me = ((sp + NY * NZ - 1) % (NY * NZ), tp)

    @pl.when(ends_row)
    def _():
        greet(nxt)

    row2, col2 = iota((256, 256), 0), iota((256, 256), 1)
    tri[...] = jnp.where((row2 > col2) & (row2 // T == col2 // T), 1.0, 0.0).astype(BF16)
    offset[...] = iota((T, 2 * T), 1) % T - iota((T, 2 * T), 0)
    acc4[...] = jnp.zeros_like(acc4)
    acc_w[...] = jnp.zeros_like(acc_w)
    sq[...] = jnp.zeros_like(sq)
    for ref in (raw, soft_b, diff, expo, weight_b):
        ref[...] = jnp.zeros_like(ref)
    qb[NZ * T :, :] = jnp.zeros((T, 128), BF16)

    pl.semaphore_wait(barrier, len(greeted) + z + jnp.where(starts_row, 1, 0))

    @pl.when(starts_row)
    def _():
        pl.semaphore_signal(ready, inc=1, device_id=before_me, device_id_type=MESH)

    loads[0].wait()

    partner = x * 2 + (1 - c)
    own_tok = tok_all.at[tp]
    tok_sends = []
    for n, d in enumerate((2, 1, 3)):
        peer = ((x + d) % NX) * 2 + c
        tok_sends.append(rcopy(own_tok, own_tok, s_a.at[n], r_a.at[tp], (sp, peer)))
    tok_sends.append(rcopy(own_tok, own_tok, s_a.at[3], r_a.at[tp], (sp, partner)))
    for send in tok_sends:
        send.start()
    for load in loads[1:8]:
        load.wait()

    def feature_step(i, _):
        dist = jnp.where(i < 2, 0, jnp.where((i == 2) | (i == 5), 1, jnp.where((i == 3) | (i == 6), 3, 2)))
        core = jnp.where((i == 1) | (i >= 5), 1 - c, c)
        src = ((x + dist) % NX) * 2 + core
        block = tok_all.at[src]

        @pl.when(i > 0)
        def _():
            rcopy(block, block, s_a.at[0], r_a.at[src], (sp, partner)).wait_recv()

        @pl.when((i >= 2) & (i <= 4))
        def _():
            rcopy(block, block, s_a.at[i + 2], r_a.at[src], (sp, partner)).start()

        feats = block[...].astype(F32)
        sq[...] += feats[:, :128] * feats[:, :128] + feats[:, 128:] * feats[:, 128:]
        at = pl.ds(pl.multiple_of(src * CH, CH), CH)
        scaled = (feats * pre_v[:, at]).astype(BF16)
        acc4[...] += dot(scaled, w4[at, :])
        acc_w[...] += dot_nt(scaled, w_win[:, at])
        return 0

    lax.fori_loop(0, NTP, feature_step, 0)
    inv = lax.rsqrt(jnp.sum(sq[...], axis=1, keepdims=True) * (1.0 / D) + EPS)

    kvb[y, 0] = (acc4[:, 0:128] * inv).T.astype(BF16)
    kvb[y, 1] = (acc4[:, 128:256] * inv).astype(BF16)
    own_kv = kvb.at[y]
    row_of = lambda d: (z * NY + (y + d) % NY, tp)
    kv_sends = []
    for plane in range(2):
        for side, d in enumerate((2, NY - 2)):
            ref = kvb.at[y, plane]
            kv_sends.append(rcopy(ref, ref, s_k.at[2 * plane + side], r_k2.at[side, plane], row_of(d)))
    for send in kv_sends:
        send.start()
    qb[rows_of(z), :] = (acc4[:, 256:384] * (inv * (0.125 * LOG2E))).astype(BF16)

    def q_send(i):
        return rcopy(qb.at[rows_of(z), :], qb.at[rows_of(z), :], s_q.at[i], r_q.at[z], (i * NY + y, tp))

    def q_start(i, _):
        q_send(i).start()
        return 0

    lax.fori_loop(0, z, q_start, 0)

    own_pair = (acc_w[...] * inv).astype(BF16)
    wkv[...] = own_pair

    @pl.when(ends_row)
    def _():
        pl.semaphore_wait(ready, 1)

    win_send = rcopy(wkv, pwkv, s_w, r_w, nxt)

    @pl.when(has_next)
    def _():
        win_send.start()

    for n, d in enumerate((1, NY - 1)):
        send = rcopy(own_kv, own_kv, s_k.at[4 + n], r_k.at[y], row_of(d))
        send.start()
        kv_sends.append(send)
    for load in loads[8:]:
        load.wait()
    pair_sends = []
    for n, ref in enumerate((wo_w.at[c], wo_s.at[c])):
        pair_sends.append(rcopy(ref, ref, s_pair.at[n], r_pair.at[n], (sp, partner)))
    for send in pair_sends:
        send.start()

    before, after = (y + NY - 2) % NY, (y + 2) % NY
    for plane in range(2):
        for side, src in enumerate((before, after)):
            ref = kvb.at[src, plane]
            rcopy(ref, ref, s_k.at[0], r_k2.at[side, plane], row_of(1)).wait_recv()
            if side == plane:
                send = rcopy(ref, ref, s_k.at[6 + side], r_k4.at[side], row_of((2, NY - 2)[side]))
                send.start()
                kv_sends.append(send)
            send = rcopy(ref, ref, s_k.at[8 + 2 * side + plane], r_k3.at[side, plane], row_of((1, NY - 1)[side]))
            send.start()
            kv_sends.append(send)

    query_w = (acc4[:, 384:512] * inv).astype(BF16)

    @pl.when(has_prev)
    def _():
        rcopy(wkv, pwkv, s_w, r_w, before_me).wait_recv()

    @pl.when(jnp.logical_not(has_prev))
    def _():
        pwkv[...] = jnp.zeros_like(pwkv)

    prev = pwkv[...]
    keys = jnp.concatenate([prev[:, :64], own_pair[:, :64]], axis=0)
    values = jnp.concatenate([prev[:, 64:], own_pair[:, 64:]], axis=0)
    q_row, k_col = iota((T, 2 * T), 0), iota((T, 2 * T), 1)
    usable = (k_col > q_row) & (k_col <= q_row + T) & ((k_col >= T) | has_prev)
    outs = []
    for h in range(2):
        logit = dot_nt(query_w[:, 64 * h : 64 * h + 64], keys) * (0.125 * LOG2E)
        logit = jnp.where(usable, logit, -jnp.inf)
        sink = sinks_s[h] * LOG2E
        top = jnp.maximum(jnp.max(logit, axis=1, keepdims=True), sink)
        weight = jnp.exp2(logit - top)
        norm = jnp.sum(weight, axis=1, keepdims=True) + jnp.exp2(sink - top)
        outs.append(dot((weight / norm).astype(BF16), values))
    win_out = jnp.concatenate(outs, axis=1).astype(BF16).astype(F32)

    def project_out(result, gain, weight, mix, inbound, buf, dst, slot, ssem, rsem):
        scaled = (result * gain[...]).astype(BF16)
        sums = split(jnp.sum(result * result, axis=1, keepdims=True))
        for core in range(2):
            for chip in range(NX):
                rows = slice(32 * chip + 16 * core, 32 * chip + 16 * core + 16)
                mix[core, 16 * chip : 16 * chip + 16, :128] = scaled[rows]
                mix[core, 16 * chip : 16 * chip + 16, 128:] = sums[rows]
        over = rcopy(mix.at[1 - c], inbound, s_pair.at[2 + slot], r_pair.at[2 + slot], (sp, partner))
        over.start()
        theirs_w = weight.at[1 - c]
        rcopy(theirs_w, theirs_w, s_pair.at[0], r_pair.at[slot], (sp, partner)).wait_recv()
        mine = mix[c, :, :128]
        own = [dot(mine, weight[c, :, n * 512 : n * 512 + 512]) for n in range(4)]
        over.wait_recv()
        theirs = inbound[:, :128]
        for n in range(4):
            part = own[n] + dot(theirs, weight[1 - c, :, n * 512 : n * 512 + 512])
            buf[:, n * 512 : n * 512 + 512] = part.astype(BF16)
        both = mix[c, :, 128:].astype(F32) + inbound[:, 128:].astype(F32)
        buf[:, D:] = split(jnp.sum(both, axis=1, keepdims=True))
        sends = []
        for d in (2, 1, 3):
            to = (x + d) % NX
            rows = buf.at[pl.ds(pl.multiple_of(to * 16, 16), 16), :]
            sends.append(rcopy(rows, dst.at[x], ssem.at[d], rsem.at[x], (sp, to * 2 + c)))
        for send in sends:
            send.start()
        return sends + [over]

    win_sends = project_out(win_out, wg_v, wo_w, mix_b, in_b, bb, rb, 0, s_rb, r_rb)

    def spread(j):
        key_t, val = kvb[j, 0], kvb[j, 1]
        zero = jnp.zeros_like(key_t)
        feat = iota((T, 128), 0) < 64
        kbd[j, :, :T] = jnp.where(feat, key_t, zero)
        kbd[j, :, T:] = jnp.where(feat, zero, key_t)
        lane = iota((T, 128), 1) < 64
        vbd[j, :T, :] = jnp.where(lane, val, zero)
        vbd[j, T:, :] = jnp.where(lane, zero, val)

    bias_row = jnp.where(iota((1, 2 * T), 1) < T, bias_s[0] * LOG2E, bias_s[1] * LOG2E)

    in_head0 = iota((2 * T, 128), 1) < 64
    far = [(y + d) % NY for d in range(NY)]
    query_pairs = (NZ - z + 1) // 2
    early = jnp.minimum(query_pairs, 2)
    units = 4 * query_pairs

    def unit(i):
        at = jnp.clip(i, 0, units - 1)
        mid, rest = at - 2 * early, jnp.maximum(at - 4 * early, 0)
        turn = early - 1 - mid // 2
        p = jnp.where(mid < 0, at // 2, jnp.where(mid < 2 * early, turn, early + rest // 4))
        k = jnp.where(mid < 0, at % 2, jnp.where(mid < 2 * early, 2 + mid % 2, rest % 4))
        real = (i >= 0) & (i < units)
        first = jnp.where(k == 0, y, jnp.where(k == 1, after, jnp.where(k == 2, far[1], far[3])))
        second = jnp.where(k == 0, before, jnp.where(k == 1, far[7], jnp.where(k == 2, far[5], far[4])))
        rows = rows_of(jnp.where(real, z + 2 * p, NZ + 1), 2)
        return p, k, real, (first, second), rows

    halves = (pl.ds(0, 2 * T), pl.ds(2 * T, 2 * T))

    def kv_wait(src):
        rcopy(kvb.at[src], kvb.at[src], s_k.at[0], r_k.at[src], row_of(1)).wait_recv()

    def await_queries(p):
        for n in range(2):
            q = z + 2 * p + n

            @pl.when((q > z) & (q < NZ))
            def _(q=q):
                block = qb.at[rows_of(q), :]
                rcopy(block, block, s_q.at[0], r_q.at[q], (q * NY + y, tp)).wait_recv()

    def total_of(q):
        rows = rows_of(q)
        part, total = parts[NY - 1, rows, :], logs[NY - 1, rows, :]
        for j in range(NY - 2, -1, -1):
            part = part + jnp.exp2(-total) * parts[j, rows, :]
            total = total + logs[j, rows, :]
        flipped = total.T
        return part, (flipped[0:1, :], flipped[64:65, :])

    def p_send(to):
        return rcopy(pout.at[to], prec.at[z], s_p.at[to], r_p.at[z], (to * NY + y, tp))

    def l_send(to):
        return rcopy(lout.at[to], lrec.at[z], s_l.at[to], r_l.at[z], (to * NY + y, tp))

    def give(zq):
        part, (l0, l1) = total_of(zq)
        pout[zq] = part.astype(BF16)
        lout[zq, 0:1, :] = l0
        lout[zq, 1:2, :] = l1
        l_send(zq).start()
        p_send(zq).start()

    def unit_step(i, now, stages=5):
        later = 1 - now
        _, _, _, pair_d, rows_d = unit(i - 4)
        for half, j in zip(halves, pair_d):
            parts[j, rows_d, :] = dot(weight_b[now, half, :], vbd[j])
        if stages >= 2:
            weight_b[later] = jnp.exp2(expo[now]).astype(BF16)
        if stages >= 3:
            expo[later] = diff[now] - dot(soft_b[now], tri[...])
        if stages >= 4:
            _, _, _, pair_b, rows_b = unit(i - 1)
            for half, j in zip(halves, pair_b):
                score = raw[now, half, :] + bias_row
                soft = jnp.maximum(score, jnp.log(1.0 + jnp.exp2(jnp.minimum(score, 126.0))) * LOG2E)
                diff[later, half, :] = score - soft
                soft_b[later, half, :] = soft.astype(BF16)
                sum0 = jnp.sum(soft[:, :T], axis=1, keepdims=True)
                sum1 = jnp.sum(soft[:, T:], axis=1, keepdims=True)
                logs[j, rows_b, :] = jnp.where(in_head0, sum0, sum1)
        if stages >= 5:
            p, _, _, pair, _ = unit(i)
            own_rows = rows_of(jnp.minimum(z + 2 * p, NZ - 1), 2)
            limit_of = lambda j: jnp.where(p == 0, (y - j) * T, NY * T)
            for half, j in zip(halves, pair):
                score = dot(qb[own_rows, :], kbd[j])
                raw[later, pl.ds(half.start, T), :] = jnp.where(offset[...] < limit_of(j), score[:T], -1e30)
                raw[later, pl.ds(half.start + T, T), :] = score[T:]

    def give_done(i):
        p_d, k_d, real_d, _, _ = unit(i)
        for n in range(2):
            q_d = z + 2 * p_d + n

            @pl.when(real_d & (k_d == 3) & (q_d > z) & (q_d < NZ))
            def _(q_d=q_d):
                give(q_d)

    def two_steps(i, _):
        first = 2 * i
        p, k, _, _, _ = unit(first)

        @pl.when((k == 0) & (first < units))
        def _():
            await_queries(p)

        @pl.when(i == 0)
        def _():
            kv_wait(far[7])
            spread(far[7])

        @pl.when(i == early)
        def _():
            kv_wait(far[1])
            spread(far[1])
            for side, src in enumerate((far[5], far[3])):
                for plane in range(2):
                    ref = kvb.at[src, plane]
                    rcopy(ref, ref, s_k.at[0], r_k3.at[side, plane], row_of(1)).wait_recv()
                spread(src)
            for n in range(2):
                rcopy(kvb.at[far[4], n], kvb.at[far[4], n], s_k.at[0], r_k4.at[n], row_of(1)).wait_recv()
            spread(far[4])

        unit_step(first, 0)
        unit_step(first + 1, 1)
        give_done(first - 3)
        return 0

    spread(y)
    spread(before)
    spread(after)
    lax.fori_loop(0, 2 * query_pairs, two_steps, 0)
    unit_step(units, 0, 4)
    unit_step(units + 1, 1, 3)
    give_done(units - 3)
    unit_step(units + 2, 0, 2)
    unit_step(units + 3, 1, 1)
    give_done(units - 1)

    own_part, own_logs = total_of(z)

    def factor_of(rows):
        spread_rows = [jnp.broadcast_to(jnp.exp2(-row), (64, 128)) for row in rows]
        return jnp.concatenate(spread_rows, axis=0).T

    acc_p[...] = jnp.zeros_like(acc_p)

    def merge(src, _):
        rcopy(lout.at[src], lrec.at[src], s_l.at[0], r_l.at[src], (src * NY + y, tp)).wait_recv()
        factor = factor_of((lrec[src, 0:1, :], lrec[src, 1:2, :]))
        rcopy(pout.at[src], prec.at[src], s_p.at[0], r_p.at[src], (src * NY + y, tp)).wait_recv()
        acc_p[...] = prec[src].astype(F32) + factor * acc_p[...]
        return 0

    lax.fori_loop(0, z, merge, 0)
    acc_p[...] = own_part + factor_of(own_logs) * acc_p[...]

    stick_out = acc_p[...].astype(BF16).astype(F32)
    stick_sends = project_out(stick_out, sg_v, wo_s, mix_a, in_a, ab, ra, 1, s_ra, r_ra)

    def gathered(buf, dst, rsem):
        total = buf[pl.ds(pl.multiple_of(x * 16, 16), 16), :].astype(F32)
        for d in (1, 3, 2):
            src = (x + d) % NX
            rcopy(dst.at[src], dst.at[src], s_ra.at[0], rsem.at[src], (sp, src * 2 + c)).wait_recv()
            total = total + dst[src].astype(F32)
        scale = lax.rsqrt(jnp.sum(total[:, D:], axis=1, keepdims=True) * (1.0 / 1024) + EPS)
        return total[:, :D] * scale

    combined = gathered(bb, rb, r_rb)
    combined = combined + gathered(ab, ra, r_ra)
    mean = jnp.sum(combined * combined, axis=1, keepdims=True) * (1.0 / D)
    out[...] = (combined * lax.rsqrt(mean + EPS) * post_v[...]).astype(BF16)

    for send in tok_sends + kv_sends + pair_sends + win_sends + stick_sends:
        send.wait_send()

    @pl.when(has_next)
    def _():
        win_send.wait_send()

    for n in (4, 5, 6):
        rcopy(own_tok, own_tok, s_a.at[n], r_a.at[tp], (sp, partner)).wait_send()

    def q_drain(i, _):
        q_send(i).wait_send()
        return 0

    lax.fori_loop(0, z, q_drain, 0)

    def p_drain(i, _):
        p_send(NZ - 1 - i).wait_send()
        l_send(NZ - 1 - i).wait_send()
        return 0

    lax.fori_loop(0, NZ - 1 - z, p_drain, 0)


def shards(
    tokens, pre_gain, w_query_stick, w_key_stick, w_value_stick, w_query_window, w_key_window, w_value_window,
    stick_bias, sinks, stick_gain, window_gain, w_out_stick, w_out_window, post_gain,
):
    anywhere = pl.BlockSpec(memory_space=pl.ANY)
    dma = pltpu.SemaphoreType.DMA
    vm = pltpu.VMEM
    scratch = [
        vm((NTP, T, CH), BF16), vm((D, 512), BF16), vm((128, D), BF16),
        vm((2, 128, D), BF16), vm((2, 128, D), BF16), vm((1, D), F32), vm((1, 128), F32), vm((1, 128), F32), vm((1, D), F32),
        vm((T, 512), F32), vm((T, 128), F32), vm((T, 128), F32),
        vm((NY, 2, T, 128), BF16), vm(((NZ + 1) * T, 128), BF16), vm((NY, 128, 2 * T), BF16), vm((NY, 2 * T, 128), BF16),
        vm((256, 256), BF16), vm((2, 4 * T, 2 * T), F32), vm((2, 4 * T, 2 * T), BF16), vm((2, 4 * T, 2 * T), F32),
        vm((2, 4 * T, 2 * T), F32), vm((2, 4 * T, 2 * T), BF16),
        vm((NY, (NZ + 3) * T, 128), F32), vm((NY, (NZ + 3) * T, 128), F32), vm((T, 2 * T), jnp.int32),
        vm((T, 128), BF16), vm((T, 128), BF16), vm((NZ, T, 128), BF16), vm((NZ, T, 128), BF16),
        vm((NZ, 2, 128), F32), vm((NZ, 2, 128), F32),
        vm((T, 128), F32), vm((64, PACK), BF16), vm((64, PACK), BF16),
        vm((NX, 16, PACK), BF16), vm((NX, 16, PACK), BF16), vm((2, 64, 256), BF16), vm((2, 64, 256), BF16),
        vm((64, 256), BF16), vm((64, 256), BF16), pltpu.SMEM((2,), F32), pltpu.SMEM((2,), F32),
        dma((15,)), dma((7,)), dma((NTP,)), dma((12,)), dma((NY,)), dma((2, 2)), dma((2, 2)), dma((2,)), dma((NZ,)), dma((NZ,)), dma, dma, pltpu.SemaphoreType.REGULAR,
        dma((NZ,)), dma((NZ,)), dma((NZ,)), dma((NZ,)), dma((NX,)), dma((NX,)), dma((NX,)), dma((NX,)), dma((4,)), dma((4,)),
    ]
    return pl.pallas_call(
        kernel,
        out_shape=jax.ShapeDtypeStruct((T // NTP, D), BF16),
        in_specs=[anywhere] * 15,
        out_specs=pl.BlockSpec(memory_space=pltpu.VMEM),
        scratch_shapes=scratch,
        compiler_params=pltpu.CompilerParams(
            collective_id=0, has_side_effects=True, vmem_limit_bytes=60 * 1024 * 1024
        ),
    )(
        tokens, pre_gain.reshape(1, -1), w_query_stick, w_key_stick, w_value_stick, w_query_window,
        w_key_window.T, w_value_window.T, stick_bias, sinks, stick_gain.reshape(1, -1), window_gain.reshape(1, -1),
        w_out_stick, w_out_window, post_gain.reshape(1, -1),
    )


def solution(mesh):
    in_specs = (
        P("sp", "tp"),
        P(),
        P(None, "tp"),
        P(None, "tp"),
        P(None, "tp"),
        P(None, "tp"),
        P(None, "tp"),
        P(None, "tp"),
        P("tp"),
        P("tp"),
        P("tp"),
        P("tp"),
        P("tp", None),
        P("tp", None),
        P(),
    )
    out_specs = P(("sp", "tp"), None)
    return jax.shard_map(shards, mesh=mesh, in_specs=in_specs, out_specs=out_specs, check_vma=False)
```
